32 devices in a mesh: sp: 8 (over z, x), tp: 4 (over y, core).
Axes of the slice: x: 2, y: 2, z: 4, core: 2. Of those that a mesh axis runs over, the one named last changes fastest.
Arguments:
- query_a: bfloat16 [1024, 2048], P('sp', 'tp'), may hold values from -6 to 6
- key_a: bfloat16 [1024, 2048], P('sp', 'tp'), may hold values from -6 to 6
- value_a: bfloat16 [1024, 4096], P('sp', 'tp'), may hold values from -6 to 6
- query_b: bfloat16 [1024, 2048], P('sp', 'tp'), may hold values from -6 to 6
- key_b: bfloat16 [1024, 2048], P('sp', 'tp'), may hold values from -6 to 6
- value_b: bfloat16 [1024, 2048], P('sp', 'tp'), may hold values from -6 to 6
- in_gate: float32 [2, 2, 16, 1024], P(None, None, 'tp', 'sp'), may hold values from -6 to 300
- forget_gate: float32 [2, 2, 16, 1024], P(None, None, 'tp', 'sp'), may hold values from 0 to 14.1
- head_gain_a: float32 [16, 256], P('tp'), may hold values from 0.1 to 1.9
- head_gain_b: float32 [16, 128], P('tp'), may hold values from 0.1 to 1.9
- out_weight_a: bfloat16 [4096, 2048], P('tp'), may hold values from -0.078125 to 0.078125
- out_weight_b: bfloat16 [2048, 2048], P('tp'), may hold values from -0.078125 to 0.078125
- residual: bfloat16 [2048, 1024], P('tp', 'sp'), may hold values from -40 to 40
- norm_gain: float32 [2048], P('tp'), may hold values from 0.1 to 1.9
- routes: int32 [1024, 2], P('sp'), may hold values from 0 to 7, all different within a row; in each aligned block of 128 rows (0 to 127, 128 to 255, ...) at most 64 rows name the same one
- route_weights: float32 [1024, 2], P('sp'), may hold values from 0.2 to 1
- expert_gate: bfloat16 [8, 2048, 4096], P('sp', None, 'tp'), may hold values from -0.125 to 0.125
- expert_up: bfloat16 [8, 2048, 4096], P('sp', None, 'tp'), may hold values from -0.125 to 0.125
- expert_down: bfloat16 [8, 4096, 2048], P('sp', 'tp'), may hold values from -0.09375 to 0.09375
Outputs:
- layer_output: bfloat16 [2048, 1024], P('tp', 'sp')
The draws below stay inside these ranges and needn't reach their ends.
Inputs may be any that keep to these rules, and one draw needn't show every extreme that they name: `routes`: each row names 2 different experts. In each aligned block of 128 rows (the rows of one index of sp) no expert is named by more than 64 rows, a bound that some blocks reach.
All inputs are finite; a program needn't handle non-finite values.
Results may differ from the reference program's by a relative error of at most 0.012.
Values may be sent and summed in bfloat16 or wider, within the bound.
A program may use at most 128 MiB of HBM per device.

```python
import math
import jax
import jax.numpy as jnp
import numpy as np
from jax import lax

D = 2048
HEAD_TOTAL = 16
DK = 128
DVA = 256
DVB = 128
BLOCK = 128
FF = 4096
TOP = 2
TOK_DEV = 128
TOKEN_TOTAL = 1024
EXPERTS = 8
SLOTS = 64
N_SP = 8
N_TP = 4


def draw_in_gate(key, part):
    base_key = jax.random.fold_in(key, 101)
    shape = (2, 2, HEAD_TOTAL, TOKEN_TOTAL)
    values = jax.random.uniform(base_key, shape, jnp.float32, -6.0, 0.0)
    return values


def draw_forget_gate(key, part):
    kind_key = jax.random.fold_in(key, 201)
    noise_key = jax.random.fold_in(key, 202)
    span_key = jax.random.fold_in(key, 203)
    spike_random_key = jax.random.fold_in(key, 204)
    depth_key = jax.random.fold_in(key, 205)
    shape = (2, 2, HEAD_TOTAL, TOKEN_TOTAL)
    spans = TOKEN_TOTAL // TOK_DEV
    quick = jax.random.randint(kind_key, (2, 2, HEAD_TOTAL, 1), 0, 2) == 1
    base = jnp.where(quick, 3.5, 11.0)
    offset = jax.random.uniform(span_key, (2, 2, HEAD_TOTAL, spans, 1), jnp.float32, -0.7, 0.7)
    offset = jnp.broadcast_to(offset, (2, 2, HEAD_TOTAL, spans, TOK_DEV)).reshape(shape)
    noise = jnp.clip(0.8 * jax.random.normal(noise_key, shape, jnp.float32), -2.4, 2.4)
    values = base + offset + noise
    spike_location = jax.random.randint(spike_random_key, (2, 2, HEAD_TOTAL, 3), 0, TOKEN_TOTAL)
    token_positions = jnp.arange(TOKEN_TOTAL, dtype=jnp.int32)
    spiked_rows = jnp.any(token_positions[None, None, None, :, None] == spike_location[:, :, :, None, :], axis=-1)
    depth = jax.random.uniform(depth_key, shape, jnp.float32, 0.0, 1.4)
    return jnp.where(spiked_rows & jnp.logical_not(quick), depth, values)


def draw_residual(key, part):
    noise_key = jax.random.fold_in(key, 301)
    scale_key = jax.random.fold_in(key, 302)
    fractions = jnp.arange(D, dtype=jnp.float32) / D
    token_scale = jnp.exp(jax.random.uniform(scale_key, (1, TOKEN_TOTAL), jnp.float32, math.log(0.3), math.log(3.0)))
    feature_scale = jnp.power(10.0, fractions - 0.5)
    values = jnp.clip(jax.random.normal(noise_key, (D, TOKEN_TOTAL), jnp.float32), -4.0, 4.0)
    return (values * feature_scale[:, None] * token_scale).astype(jnp.bfloat16)


def shard_levels(rng, extent, cuts, least, largest):
    gain = 1.0
    for axis_at, blocks in cuts:
        heights = jax.random.uniform(jax.random.fold_in(jax.random.fold_in(rng, 6), axis_at), (blocks,), jnp.float32, least / len(cuts), largest / len(cuts))
        gain = gain * jnp.repeat(jnp.exp(heights), extent[axis_at] // blocks).reshape((-1,) + (1,) * (len(extent) - 1 - axis_at))
    return gain


def deal_out(key, own, number, rows, count, top, reach, skew):
    sequence = jax.random.permutation(key, count)
    packed, common = shares(count, rows * top, reach, skew, True), shares(count, rows * top, reach, skew, False)
    places = jnp.arange(count)

    def named(tallies, rotation):
        used = int((tallies > 0).sum())
        fixed = max(1, used // 4)
        passed = fixed + (places - fixed + rotation * (used - fixed)) % max(1, count - fixed)
        return jnp.zeros((count,), jnp.int32).at[sequence[jnp.where(places < fixed, places, passed)]].set(jnp.asarray(tallies, jnp.int32))

    tallies = jnp.where(number % 4 == 0, named(packed, number // 4), named(common, number - number // 4 - 1))
    mixed = jax.random.permutation(jax.random.fold_in(own, 3), count)
    source_of, receiver = mixed[0:count // 2 * 2:2], mixed[1:count // 2 * 2:2]
    margin = jnp.minimum(tallies[source_of] - 1, reach - tallies[receiver]) // 2
    margin = jnp.where((source_of == sequence[0]) | (receiver == sequence[0]) | (tallies[receiver] == 0), 0, jnp.maximum(margin, 0))
    passed = jax.random.randint(jax.random.fold_in(own, 4), (count // 2,), 0, 1 << 20) % (margin + 1)
    tallies = tallies.at[source_of].add(-passed).at[receiver].add(passed)
    labels = jnp.searchsorted(jnp.cumsum(tallies), jnp.arange(rows * top), side="right").astype(jnp.int32)
    grid = labels.reshape(top, rows).T
    grid = grid[jax.random.permutation(jax.random.fold_in(own, 1), rows)]
    rotation = jax.random.randint(jax.random.fold_in(own, 2), (rows, 1), 0, top)
    return jnp.take_along_axis(grid, (jnp.arange(top)[None, :] + rotation) % top, axis=1)


def shares(count, total, limit, lean, full):
    loads = [(1 << 20) // math.isqrt(rank ** lean) + 1 for rank in range(1, count + 1)]
    largest = limit if full else min(limit, max(-(-total // count), total * loads[0] // sum(loads)))
    least = 1 if total - largest >= count - 1 else 0
    counts, surplus = [largest] + [least] * (count - 1), total - largest - least * (count - 1)
    while surplus > 0:
        candidates = [i for i in range(1, count) if counts[i] < largest] or [i for i in range(1, count) if counts[i] < limit]
        pool, remaining = sum([loads[i] for i in candidates]), surplus
        for i in candidates:
            addition = min(limit - counts[i], max(1, remaining * loads[i] // pool), surplus)
            counts[i] = counts[i] + addition
            surplus = surplus - addition
    return np.array(counts)


def scatter_about(own_key, extent, scale, most, cuts=(), held_as=jnp.bfloat16):
    drawn = jax.random.normal(own_key, extent, jnp.float32) * scale
    if len(cuts) > 0:
        drawn = shard_levels(own_key, extent, cuts, -0.22, 0.18) * drawn
    return jnp.clip(drawn, min=-most, max=most).astype(held_as)


def setup_inputs(seed: int = 0) -> dict:
    keys = jax.random.split(jax.random.key(seed), 20)
    query_a = scatter_about(keys[0], (TOKEN_TOTAL, HEAD_TOTAL * DK), 1.0, 6.0, ((0, 8), (1, 4)))
    key_a = scatter_about(keys[1], (TOKEN_TOTAL, HEAD_TOTAL * DK), 1.0, 6.0, ((0, 8), (1, 4)))
    value_a = scatter_about(keys[2], (TOKEN_TOTAL, HEAD_TOTAL * DVA), 1.0, 6.0, ((0, 8), (1, 4)))
    query_b = scatter_about(keys[3], (TOKEN_TOTAL, HEAD_TOTAL * DK), 1.0, 6.0, ((0, 8), (1, 4)))
    key_b = scatter_about(keys[4], (TOKEN_TOTAL, HEAD_TOTAL * DK), 1.0, 6.0, ((0, 8), (1, 4)))
    value_b = scatter_about(keys[5], (TOKEN_TOTAL, HEAD_TOTAL * DVB), 1.0, 6.0, ((0, 8), (1, 4)))
    in_gate = draw_in_gate(jax.random.fold_in(keys[19], 71), 0)
    forget_gate = draw_forget_gate(jax.random.fold_in(keys[19], 71), 0)
    head_gain_a = jnp.clip(1.0 + 0.18 * jax.random.normal(keys[8], (HEAD_TOTAL, DVA), jnp.float32), 0.1, 1.9)
    head_gain_b = jnp.clip(1.0 + 0.18 * jax.random.normal(keys[9], (HEAD_TOTAL, DVB), jnp.float32), 0.1, 1.9)
    out_weight_a = scatter_about(keys[10], (HEAD_TOTAL * DVA, D), (HEAD_TOTAL * (DVA + DVB)) ** -0.5, 0.078125, ((0, 4),))
    out_weight_b = scatter_about(keys[11], (HEAD_TOTAL * DVB, D), (HEAD_TOTAL * (DVA + DVB)) ** -0.5, 0.078125, ((0, 4),))
    residual = draw_residual(jax.random.fold_in(keys[19], 71), 0)
    norm_gain = jnp.clip(1.0 + 0.18 * jax.random.normal(keys[13], (D,), jnp.float32), 0.1, 1.9)
    routes_keys = jax.random.split(jax.random.fold_in(keys[14], 1), TOKEN_TOTAL // TOK_DEV)
    routes_turns = jax.random.permutation(jax.random.fold_in(keys[14], 3), TOKEN_TOTAL // TOK_DEV)
    routes = jax.vmap(lambda own, number: deal_out(jax.random.fold_in(keys[14], 2), own, number, TOK_DEV, EXPERTS, TOP, SLOTS, 3))(routes_keys, routes_turns).reshape((TOKEN_TOTAL, TOP))
    route_weights = jnp.clip(0.2 + 0.8 * jax.random.uniform(keys[15], (TOKEN_TOTAL, TOP), jnp.float32) ** shard_levels(keys[15], (TOKEN_TOTAL, TOP), ((0, 8),), -0.2, 0.2), 0.2, 1.0)
    expert_gate = scatter_about(keys[16], (EXPERTS, D, FF), D ** -0.5, 0.125, ((0, 8), (2, 4)))
    expert_up = scatter_about(keys[17], (EXPERTS, D, FF), D ** -0.5, 0.125, ((0, 8), (2, 4)))
    expert_down = scatter_about(keys[18], (EXPERTS, FF, D), FF ** -0.5, 0.09375, ((0, 8), (1, 4)))
    return dict(query_a=query_a, key_a=key_a, value_a=value_a, query_b=query_b, key_b=key_b, value_b=value_b, in_gate=in_gate, forget_gate=forget_gate, head_gain_a=head_gain_a, head_gain_b=head_gain_b, out_weight_a=out_weight_a, out_weight_b=out_weight_b, residual=residual, norm_gain=norm_gain, routes=routes, route_weights=route_weights, expert_gate=expert_gate, expert_up=expert_up, expert_down=expert_down)


EPSILON = 1e-06

def one_direction(queries, keys_in, values_in, log_input, log_decay):
    head_count, length, width_k = queries.shape
    blocks = length // BLOCK
    lower_mask = jnp.tril(jnp.ones((BLOCK, BLOCK), dtype=bool))

    def to_blocks(tensor):
        return jnp.moveaxis(tensor.reshape(head_count, blocks, BLOCK, *tensor.shape[2:]), 1, 0)

    def block_step(carried_state, inputs_block):
        memory, normal, stabilizer = carried_state
        q_block, k_block, v_block, in_block, decay_block = inputs_block
        cumulative = jnp.cumsum(decay_block, axis=-1)
        running_log_decay = cumulative + stabilizer[:, None]
        log_weights = jnp.where(lower_mask, cumulative[:, :, None] - cumulative[:, None, :] + in_block[:, None, :], -jnp.inf)
        row_peak = jnp.maximum(running_log_decay, lax.optimization_barrier(jnp.max(log_weights, axis=-1)))
        carried_weight = jnp.exp(running_log_decay - row_peak)
        scores = jnp.einsum('htd,hsd->hts', q_block, k_block) * jnp.exp(log_weights - row_peak[:, :, None])
        rounded = lax.optimization_barrier(scores.astype(jnp.bfloat16)).astype(jnp.float32)
        numerator = carried_weight[:, :, None] * jnp.einsum('htd,hde->hte', q_block, memory) + jnp.einsum('hts,hse->hte', rounded, v_block)
        denominator = carried_weight * jnp.einsum('htd,hd->ht', q_block, normal) + lax.optimization_barrier(jnp.sum(scores, axis=-1))
        outputs = numerator / jnp.maximum(jnp.abs(denominator), jnp.exp(-row_peak))[:, :, None]
        decay_total = cumulative[:, -1]
        tail_logs = decay_total[:, None] - cumulative + in_block
        new_stabilizer = jnp.maximum(decay_total + stabilizer, lax.optimization_barrier(jnp.max(tail_logs, axis=-1)))
        keep_scale = jnp.exp(decay_total + stabilizer - new_stabilizer)
        weighted_keys = k_block * jnp.exp(tail_logs - new_stabilizer[:, None])[:, :, None]
        memory = keep_scale[:, None, None] * memory + jnp.einsum('hsd,hse->hde', weighted_keys, v_block)
        normal = keep_scale[:, None] * normal + lax.optimization_barrier(jnp.sum(weighted_keys, axis=1))
        return ((memory, normal, new_stabilizer), outputs)
    start = (jnp.zeros((head_count, width_k, values_in.shape[-1]), jnp.float32), jnp.zeros((head_count, width_k), jnp.float32), jnp.zeros((head_count,), jnp.float32))
    blocked = tuple((to_blocks(tensor) for tensor in (queries, keys_in, values_in, log_input, log_decay)))
    final_state, outputs = lax.scan(block_step, start, blocked)
    return jnp.moveaxis(outputs, 0, 1).reshape(head_count, length, -1)

def mixer_group(queries, keys_in, values_in, log_input, log_decay, head_gain):
    width_k = queries.shape[1] // HEAD_TOTAL
    width_v = values_in.shape[1] // HEAD_TOTAL
    q_heads = queries.astype(jnp.float32).reshape(TOKEN_TOTAL, HEAD_TOTAL, width_k).transpose(1, 0, 2) * width_k ** (-0.5)
    k_heads = keys_in.astype(jnp.float32).reshape(TOKEN_TOTAL, HEAD_TOTAL, width_k).transpose(1, 0, 2)
    v_heads = values_in.astype(jnp.float32).reshape(TOKEN_TOTAL, HEAD_TOTAL, width_v).transpose(1, 0, 2)
    forward = one_direction(q_heads, k_heads, v_heads, log_input[0], log_decay[0])
    backward = jnp.flip(one_direction(jnp.flip(q_heads, 1), jnp.flip(k_heads, 1), jnp.flip(v_heads, 1), jnp.flip(log_input[1], 1), jnp.flip(log_decay[1], 1)), 1)
    both = forward + backward
    scaled = both * lax.rsqrt(lax.optimization_barrier(jnp.mean(both * both, axis=-1, keepdims=True)) + EPSILON) * head_gain[:, None, :]
    return scaled.astype(jnp.bfloat16).transpose(1, 0, 2).reshape(TOKEN_TOTAL, HEAD_TOTAL * width_v)

def reference(query_a, key_a, value_a, query_b, key_b, value_b, in_gate, forget_gate, head_gain_a, head_gain_b, out_weight_a, out_weight_b, residual, norm_gain, routes, route_weights, expert_gate, expert_up, expert_down):
    log_decay = jax.nn.log_sigmoid(forget_gate)
    heads_a = mixer_group(query_a, key_a, value_a, in_gate[:, 0], log_decay[:, 0], head_gain_a)
    heads_b = mixer_group(query_b, key_b, value_b, in_gate[:, 1], log_decay[:, 1], head_gain_b)
    mix = jnp.dot(heads_a, out_weight_a, preferred_element_type=jnp.float32) + jnp.dot(heads_b, out_weight_b, preferred_element_type=jnp.float32)
    updated = residual.astype(jnp.float32) + mix.T
    squares = lax.optimization_barrier(jnp.sum(updated * updated, axis=0))
    normed = (updated * lax.rsqrt(squares / D + EPSILON)[None, :] * norm_gain[:, None]).astype(jnp.bfloat16)
    token_rows = normed.T
    flat_routes = routes.reshape(N_SP, TOK_DEV * TOP)
    hits = (flat_routes[:, :, None] == jnp.arange(EXPERTS, dtype=jnp.int32)[None, None, :]).astype(jnp.int32)
    ranks = lax.optimization_barrier(jnp.sum((jnp.cumsum(hits, axis=1) - 1) * hits, axis=2))
    token_positions = (jnp.arange(N_SP, dtype=jnp.int32)[:, None] * SLOTS + ranks).reshape(TOKEN_TOTAL, TOP).astype(jnp.int32)
    owners = jnp.broadcast_to(jnp.arange(TOKEN_TOTAL, dtype=jnp.int32)[:, None], (TOKEN_TOTAL, TOP))
    table = jnp.zeros((EXPERTS, N_SP * SLOTS), jnp.int32).at[routes, token_positions].set(owners)
    group_width = FF // N_TP

    def one_expert(inputs_expert):
        gate_matrix, up_matrix, down_matrix, row_ids = inputs_expert
        rows = jnp.take(token_rows, row_ids, axis=0)
        gate = jnp.dot(rows, gate_matrix, preferred_element_type=jnp.float32)
        upward = jnp.dot(rows, up_matrix, preferred_element_type=jnp.float32)
        hidden = (jax.nn.silu(gate) * upward).astype(jnp.bfloat16)
        pieces = jnp.einsum('rjg,jgd->jrd', hidden.reshape(-1, N_TP, group_width).astype(jnp.float32), down_matrix.reshape(N_TP, group_width, D).astype(jnp.float32))
        pieces = lax.optimization_barrier(pieces.astype(jnp.bfloat16)).astype(jnp.float32)
        return lax.optimization_barrier(jnp.sum(pieces, axis=0)).astype(jnp.bfloat16)
    expert_rows = lax.map(one_expert, (expert_gate, expert_up, expert_down, table))
    picked = expert_rows[routes, token_positions].astype(jnp.float32)
    combined = updated + lax.optimization_barrier(jnp.sum(route_weights[:, :, None] * picked, axis=1)).T
    return combined.astype(jnp.bfloat16)
```

```python
import functools

import jax
import jax.numpy as jnp
from jax import lax
from jax.experimental import pallas as pl
from jax.experimental.pallas import tpu as pltpu
from jax.sharding import PartitionSpec as P

EPSILON = 1e-06
NOTHING = -1e30


def dot(left, right, contract):
    return lax.dot_general(
        left, right, (contract, ((), ())), preferred_element_type=jnp.float32
    )


MESH = pl.DeviceIdType.MESH


def greet(peers):
    barrier = pltpu.get_barrier_semaphore()
    for peer in peers:
        pl.semaphore_signal(barrier, inc=1, device_id=peer, device_id_type=MESH)
    pl.semaphore_wait(barrier, len(peers))


def exchange_kernel(count, arrays, *refs):
    given, taken = refs[:arrays], refs[arrays : 2 * arrays]
    sent, landed, kept = refs[2 * arrays :]
    mine = lax.axis_index("sp")
    peers = [lax.rem(mine + step, count) for step in range(1, count)]
    greet([{"sp": peer} for peer in peers])
    copies = []
    for step, peer in enumerate(peers):
        for a in range(arrays):
            copy = pltpu.make_async_remote_copy(
                src_ref=given[a].at[peer],
                dst_ref=taken[a].at[mine],
                send_sem=sent.at[a, step],
                recv_sem=landed.at[a, step],
                device_id={"sp": peer},
                device_id_type=MESH,
            )
            copy.start()
            copies.append(copy)
    for a in range(arrays):
        copy = pltpu.make_async_copy(given[a].at[mine], taken[a].at[mine], kept.at[a])
        copy.start()
        copies.append(copy)
    for copy in copies:
        copy.wait()


def exchange(arrays, number):
    count = arrays[0].shape[0]
    spec = pl.BlockSpec(memory_space=pltpu.VMEM)
    return pl.pallas_call(
        functools.partial(exchange_kernel, count, len(arrays)),
        out_shape=[jax.ShapeDtypeStruct(a.shape, a.dtype) for a in arrays],
        in_specs=[spec] * len(arrays),
        out_specs=[spec] * len(arrays),
        scratch_shapes=[
            pltpu.SemaphoreType.DMA((len(arrays), count - 1)),
            pltpu.SemaphoreType.DMA((len(arrays), count - 1)),
            pltpu.SemaphoreType.DMA((len(arrays),)),
        ],
        compiler_params=pltpu.CompilerParams(collective_id=number, has_side_effects=True),
    )(*arrays)


def moe_kernel(
    count, across, given, gate_hbm, up_hbm, down_hbm, out,
    rows, gate_w, up_w, down_w, hidden, part, partner, chip, cross, total,
    kept, weight, sent, landed, y_sent, y_landed, c_sent, c_landed,
    t_sent, t_landed, r_sent, r_landed, s_sent, s_landed,
):
    mine, slot = lax.axis_index("sp"), lax.axis_index("tp")
    chips = across // 2
    slots, width = given.shape[1], given.shape[2]
    units = gate_w.shape[1]
    core = lax.rem(slot, 2)
    row = lax.div(slot, 2)
    twin = slot + 1 - 2 * core
    others = [lax.rem(slot + 2 * step, across) for step in range(1, chips)]
    behind = [lax.rem(slot + across - 2 * step, across) for step in range(1, chips)]
    weights = [
        pltpu.make_async_copy(source, target, weight.at[i])
        for i, (source, target) in enumerate(
            ((gate_hbm, gate_w), (up_hbm, up_w), (down_hbm, down_w))
        )
    ]
    for copy in weights:
        copy.start()
    targets = [lax.rem(mine + step, count) for step in range(count)]
    sources = [lax.rem(mine + count - step, count) for step in range(count)]
    greet(
        [{"sp": target} for target in targets[1:]]
        + [{"tp": other} for other in others]
        + [{"tp": twin}]
    )

    def remote(source, target, send, land, device):
        copy = pltpu.make_async_remote_copy(
            src_ref=source, dst_ref=target, send_sem=send, recv_sem=land,
            device_id=device, device_id_type=MESH,
        )
        copy.start()
        return copy

    def place(step, owner):
        return rows.at[step, :, pl.ds(pl.multiple_of(owner * width, width), width)]

    first = [pltpu.make_async_copy(given.at[mine], place(0, slot), kept.at[0])]
    first[0].start()
    for step in range(1, count):
        first.append(
            remote(
                given.at[targets[step]], place(step, slot), sent.at[step], landed.at[step],
                {"sp": targets[step]},
            )
        )
    along = {}
    last = {}

    def relay(step):
        if step == 0:
            first[0].wait()
        else:
            first[step].wait_recv()
        along[step] = [
            remote(
                place(step, slot), place(step, slot),
                y_sent.at[step, turn], y_landed.at[step, turn], {"tp": other},
            )
            for turn, other in enumerate(others)
        ]
        last[step] = [
            remote(
                place(step, slot), place(step, slot),
                c_sent.at[step, 0], c_landed.at[step, 0], {"tp": twin},
            )
        ]

    def hand_over(step):
        for turn, owner in enumerate(behind):
            along[step][turn].wait_recv()
            last[step].append(
                remote(
                    place(step, owner), place(step, owner),
                    c_sent.at[step, turn + 1], c_landed.at[step, turn + 1], {"tp": twin},
                )
            )

    half = count // 2
    tile = min(256, units)
    batch = half * slots

    def arrive(steps):
        for step in steps:
            for copy in last[step]:
                copy.wait_recv()

    def lift(h, turns):
        x = rows[h * half : (h + 1) * half].reshape(batch, width * across)
        for turn in turns:
            columns = slice(turn * tile, (turn + 1) * tile)
            gate = dot(x, gate_w[:, columns], ((1,), (0,)))
            upward = dot(x, up_w[:, columns], ((1,), (0,)))
            hidden[h * batch : (h + 1) * batch, columns] = (
                jax.nn.silu(gate) * upward
            ).astype(jnp.bfloat16)

    def lower(h, owners):
        x = hidden[h * batch : (h + 1) * batch, :]
        for owner in owners:
            y = dot(x, down_w[:, owner * width : (owner + 1) * width], ((1,), (0,)))
            part[owner, h * half : (h + 1) * half] = y.astype(jnp.bfloat16).reshape(
                half, slots, width
            )

    pieces = 2
    span = half // pieces
    over, crossed, back = {}, {}, {}

    def group(h, piece):
        return pl.ds(h * half + piece * span, span)

    def pass_twin(h):
        for piece in range(pieces):
            for y in range(chips):
                block = group(h, piece)
                over[h, piece, y] = remote(
                    part.at[2 * y + 1 - core, block], partner.at[y, block],
                    t_sent.at[h * pieces + piece, y], t_landed.at[h * pieces + piece, y],
                    {"tp": twin},
                )

    def join_twin(h, piece):
        block = group(h, piece)
        for y in range(chips):
            over[h, piece, y].wait_recv()
        for turn in range(chips - 1):
            y = lax.rem(row + turn + 1, chips)
            chip[turn, block] = (
                part[2 * y + core, block].astype(jnp.float32)
                + partner[y, block].astype(jnp.float32)
            ).astype(jnp.bfloat16)
            crossed[h, piece, turn] = remote(
                chip.at[turn, block], cross.at[turn, block],
                r_sent.at[h * pieces + piece, turn], r_landed.at[h * pieces + piece, turn],
                {"tp": others[turn]},
            )

    def give_back(h, piece):
        block = group(h, piece)
        value = part[2 * row + core, block].astype(jnp.float32) + partner[row, block].astype(
            jnp.float32
        )
        for turn in range(chips - 1):
            crossed[h, piece, turn].wait_recv()
            value = value + cross[turn, block].astype(jnp.float32)
        total[block] = value.astype(jnp.bfloat16)
        for step in range(h * half + piece * span, h * half + (piece + 1) * span):
            if step == 0:
                back[step] = pltpu.make_async_copy(total.at[0], out.at[mine], kept.at[1])
                back[step].start()
            else:
                back[step] = remote(
                    total.at[step], out.at[mine], s_sent.at[step], s_landed.at[step],
                    {"sp": sources[step]},
                )

    turns = list(range(units // tile))
    cut = half + 1
    relay(0)
    for step in range(1, cut):
        relay(step)
        hand_over(step - 1)
    weights[0].wait()
    weights[1].wait()
    arrive(range(half))
    rest = list(range(cut, count))
    work = [functools.partial(lift, 0, [turn]) for turn in turns]
    work.append(weights[2].wait)
    work += [functools.partial(lower, 0, [owner]) for owner in range(across)]
    work.append(functools.partial(pass_twin, 0))
    share = -(-len(work) // (len(rest) + 1))
    for at in range(len(rest) + 1):
        for thunk in work[at * share : (at + 1) * share]:
            thunk()
        if at < len(rest):
            relay(rest[at])
            hand_over(rest[at] - 1)
    hand_over(count - 1)
    for piece in range(pieces):
        join_twin(0, piece)
    arrive(range(half, count))
    lift(1, turns)
    for piece in range(pieces):
        give_back(0, piece)
    lower(1, range(across))
    pass_twin(1)
    for piece in range(pieces):
        join_twin(1, piece)
    for piece in range(pieces):
        give_back(1, piece)
    for step in range(count):
        if step == 0:
            back[0].wait()
        else:
            first[step].wait_send()
            back[step].wait()
        for copy in along[step]:
            copy.wait_send()
        for copy in last[step]:
            copy.wait_send()
    for copy in list(over.values()) + list(crossed.values()):
        copy.wait_send()


def moe(given, gate, up, down, number):
    count, slots, width = given.shape
    across = lax.axis_size("tp")
    chips = across // 2
    units = gate.shape[1]
    vmem = pl.BlockSpec(memory_space=pltpu.VMEM)
    whole = pl.BlockSpec(memory_space=pl.ANY)
    dma = pltpu.SemaphoreType.DMA
    bf16 = jnp.bfloat16
    pieces = 4
    return pl.pallas_call(
        functools.partial(moe_kernel, count, across),
        out_shape=jax.ShapeDtypeStruct((count, slots, width), bf16),
        in_specs=[vmem, whole, whole, whole],
        out_specs=vmem,
        scratch_shapes=[
            pltpu.VMEM((count, slots, width * across), bf16),
            pltpu.VMEM(gate.shape, bf16),
            pltpu.VMEM(up.shape, bf16),
            pltpu.VMEM(down.shape, bf16),
            pltpu.VMEM((count * slots, units), bf16),
            pltpu.VMEM((across, count, slots, width), bf16),
            pltpu.VMEM((chips, count, slots, width), bf16),
            pltpu.VMEM((chips - 1, count, slots, width), bf16),
            pltpu.VMEM((chips - 1, count, slots, width), bf16),
            pltpu.VMEM((count, slots, width), bf16),
            dma((2,)), dma((3,)),
            dma((count,)), dma((count,)),
            dma((count, chips - 1)), dma((count, chips - 1)),
            dma((count, chips)), dma((count, chips)),
            dma((pieces, chips)), dma((pieces, chips)),
            dma((pieces, chips - 1)), dma((pieces, chips - 1)),
            dma((count,)), dma((count,)),
        ],
        compiler_params=pltpu.CompilerParams(
            collective_id=number, has_side_effects=True, vmem_limit_bytes=48 * 1024 * 1024
        ),
    )(given, gate, up, down)


def one_head(query, key, value, keys, values, inner_row, outer_row, column, peak, gain, share):
    length, width_k = query.shape
    scale = width_k ** (-0.5)
    rows = lax.broadcasted_iota(jnp.int32, (length, length), 0)
    lanes = lax.broadcasted_iota(jnp.int32, (length, length), 1)
    near = dot(query, key, ((1,), (1,))) * scale
    far = dot(query, keys, ((1,), (1,))) * scale
    far_scores = [far * outer_row[r] for r in range(2)]
    far_sums = [jnp.sum(scores, axis=1, keepdims=True) for scores in far_scores]
    far_values = dot(
        jnp.concatenate([scores.astype(jnp.bfloat16) for scores in far_scores], axis=0),
        values,
        ((1,), (0,)),
    )
    both = None
    for r in range(2):
        keep = lanes <= rows if r == 0 else lanes >= rows
        logs = jnp.where(keep, column[r] + inner_row[r], NOTHING)
        carried_log = column[r] + peak[r]
        top = jnp.maximum(carried_log, jnp.max(logs, axis=1, keepdims=True))
        carried = jnp.exp(carried_log - top)
        scores = near * jnp.exp(logs - top)
        numer = carried * far_values[r * length : (r + 1) * length] + dot(
            scores.astype(jnp.bfloat16), value, ((1,), (0,))
        )
        denom = carried * far_sums[r] + jnp.sum(scores, axis=1, keepdims=True)
        out = numer / jnp.maximum(jnp.abs(denom), jnp.exp(-top))
        both = out if both is None else both + out
    mean = jnp.sum(both * both, axis=1, keepdims=True) * share
    return (both * lax.rsqrt(mean + EPSILON) * gain).astype(jnp.bfloat16)


def mixer_kernel(
    qa, ka, va, qb, kb, vb, all_ka, all_va, all_kb, all_vb,
    inner, outer, column, peak, gain_a, gain_b, heads_a, heads_b,
):
    parts = (
        (qa, ka, va, all_ka, all_va, gain_a, heads_a),
        (qb, kb, vb, all_kb, all_vb, gain_b, heads_b),
    )
    for g, (q, k, v, every_k, every_v, gain, heads) in enumerate(parts):
        heads[...] = one_head(
            q[...], k[...], v[...], every_k[...], every_v[...],
            [inner[0, 2 * r + g : 2 * r + g + 1, :] for r in range(2)],
            [outer[0, 2 * r + g : 2 * r + g + 1, :] for r in range(2)],
            [column[0, :, 2 * r + g : 2 * r + g + 1] for r in range(2)],
            [peak[0, 2 * r + g : 2 * r + g + 1, 0:1] for r in range(2)],
            gain[0],
            1.0 / gain.shape[-1],
        )


def mix_heads(query_a, key_a, value_a, query_b, key_b, value_b, in_gate, forget_gate, gain_a, gain_b):
    heads = gain_a.shape[0]
    length = query_a.shape[0]
    width_k = query_a.shape[1] // heads
    width_a, width_b = gain_a.shape[1], gain_b.shape[1]
    count, mine = lax.axis_size("sp"), lax.axis_index("sp")
    packed = jnp.concatenate([value_a, key_a, key_b, value_b], axis=1)
    gathered = lax.all_gather(packed, "sp", axis=0, tiled=True)
    total_rows = gathered.shape[0]
    log_decay = jax.nn.log_sigmoid(forget_gate)
    ones = jnp.ones((length, length), jnp.float32)
    exact = lax.Precision.HIGHEST
    run = jnp.stack(
        [
            jnp.einsum("ghs,st->ght", log_decay[0], jnp.triu(ones), precision=exact),
            jnp.einsum("ghs,st->ght", log_decay[1], jnp.tril(ones), precision=exact),
        ]
    )
    whole = jnp.sum(log_decay, axis=-1, keepdims=True)
    tails = in_gate + whole - run
    small = lax.all_gather(
        jnp.stack([tails, jnp.broadcast_to(whole, tails.shape)]), "sp", axis=0
    )
    every_tail, every_whole = small[:, 0], small[:, 1, ..., 0]
    place = jnp.arange(count)
    source, middle = place[:, None], place[None, :]
    between = jnp.stack(
        [
            (middle > source) & (middle < mine),
            (middle < source) & (middle > mine),
        ]
    ).astype(jnp.float32)
    gap = jnp.sum(between[:, :, :, None, None] * jnp.moveaxis(every_whole, 0, 1)[:, None], axis=2)
    seen = jnp.stack([place < mine, place > mine])[:, :, None, None, None]
    logs = jnp.where(seen, jnp.moveaxis(every_tail, 0, 1) + gap[..., None], NOTHING)
    peak = jnp.max(logs, axis=(1, 4))
    outer = jnp.where(seen, jnp.exp(logs - peak[:, None, :, :, None]), 0.0)
    outer = outer.transpose(3, 0, 2, 1, 4).reshape(heads, 4, total_rows)
    peak = jnp.broadcast_to(peak.transpose(2, 0, 1).reshape(heads, 4, 1), (heads, 4, 128))
    inner = (in_gate - run).transpose(2, 0, 1, 3).reshape(heads, 4, length)
    column = run.transpose(2, 3, 0, 1).reshape(heads, length, 4)
    ratio = width_a // width_k

    def columns(rows, width, first):
        return pl.BlockSpec((rows, width), lambda h: (0, first + h))

    def by_head(*shape):
        return pl.BlockSpec((1,) + shape, lambda h: (h, 0, 0))

    return pl.pallas_call(
        mixer_kernel,
        grid=(heads,),
        in_specs=[
            columns(length, width_k, 0),
            columns(length, width_k, 0),
            columns(length, width_a, 0),
            columns(length, width_k, 0),
            columns(length, width_k, 0),
            columns(length, width_b, 0),
            columns(total_rows, width_k, ratio * heads),
            columns(total_rows, width_a, 0),
            columns(total_rows, width_k, (ratio + 1) * heads),
            columns(total_rows, width_b, (ratio + 2) * heads),
            by_head(4, length),
            by_head(4, total_rows),
            by_head(length, 4),
            by_head(4, 128),
            by_head(1, width_a),
            by_head(1, width_b),
        ],
        out_specs=[columns(length, width_a, 0), columns(length, width_b, 0)],
        out_shape=[
            jax.ShapeDtypeStruct((length, heads * width_a), jnp.bfloat16),
            jax.ShapeDtypeStruct((length, heads * width_b), jnp.bfloat16),
        ],
        cost_estimate=pl.CostEstimate(
            flops=4 * heads * length * total_rows * (2 * width_k + 2 * width_a),
            bytes_accessed=2 * packed.size * count,
            transcendentals=0,
        ),
    )(
        query_a, key_a, value_a, query_b, key_b, value_b,
        gathered, gathered, gathered, gathered,
        inner, outer, column, peak, gain_a[:, None, :], gain_b[:, None, :],
    )


def unit_kernel(q, k, v, every_k, every_v, inner, outer, column, peak, gain, share, heads):
    heads[0] = one_head(
        q[0], k[0], v[0], every_k[...].reshape(-1, every_k.shape[-1]),
        every_v[...].reshape(-1, every_v.shape[-1]),
        [inner[0, r : r + 1, :] for r in range(2)],
        [outer[0, r : r + 1, :] for r in range(2)],
        [column[0, :, r : r + 1] for r in range(2)],
        [peak[0, r : r + 1, 0:1] for r in range(2)],
        gain[...],
        share[0:1, 0:1],
    )


def mix_units(query_a, key_a, value_a, query_b, key_b, value_b, in_gate, forget_gate, gain_a, gain_b):
    heads = gain_a.shape[0]
    length = query_a.shape[0]
    width_k = query_a.shape[1] // heads
    width_a, width_b = gain_a.shape[1], gain_b.shape[1]
    count, mine = lax.axis_size("sp"), lax.axis_index("sp")

    def widen(array, axis):
        pads = [(0, 0)] * array.ndim
        pads[axis] = (0, width_a - width_b)
        return jnp.pad(array, pads)

    def cut(values, queries, keys, width):
        parts = []
        for h in range(heads):
            value = values[:, h * width : (h + 1) * width]
            parts.append(
                jnp.concatenate(
                    [
                        value if width == width_a else widen(value, 1),
                        queries[:, h * width_k : (h + 1) * width_k],
                        keys[:, h * width_k : (h + 1) * width_k],
                    ],
                    axis=1,
                )
            )
        return parts

    packed = jnp.stack(
        cut(value_a, query_a, key_a, width_a) + cut(value_b, query_b, key_b, width_b)
    )
    log_decay = jax.nn.log_sigmoid(forget_gate)
    gates = jnp.stack([in_gate, log_decay], axis=2)
    gates = gates.transpose(1, 3, 0, 2, 4).reshape(count, 4, length)
    gates = jnp.concatenate([gates, jnp.zeros_like(gates)], axis=1)
    rows, gates = exchange([packed, gates], 0)
    in_rows, decay = gates[:, 0:4:2], gates[:, 1:4:2]
    ones = jnp.ones((length, length), jnp.float32)
    exact = lax.Precision.HIGHEST
    run = jnp.stack(
        [
            jnp.dot(decay[:, 0], jnp.triu(ones), precision=exact),
            jnp.dot(decay[:, 1], jnp.tril(ones), precision=exact),
        ],
        axis=1,
    )
    whole = jnp.sum(decay, axis=-1)
    tails = in_rows + whole[..., None] - run
    place = jnp.arange(count)
    reader, source, middle = place[:, None, None], place[None, :, None], place[None, None, :]
    between = jnp.stack(
        [
            (middle > source) & (middle < reader),
            (middle < source) & (middle > reader),
        ],
        axis=1,
    ).astype(jnp.float32)
    gap = jnp.sum(between * whole.T[None, :, None, :], axis=-1)
    seen = jnp.stack([source < reader, source > reader], axis=1)
    logs = jnp.where(seen, tails.transpose(1, 0, 2)[None] + gap[..., None], NOTHING)
    peak = jnp.max(logs, axis=(2, 3))
    outer = jnp.where(seen, jnp.exp(logs - peak[:, :, None, None]), 0.0)
    outer = outer.reshape(count, 2, count * length)
    peak = jnp.broadcast_to(peak[:, :, None], (count, 2, 128))
    inner = in_rows - run
    column = run.transpose(0, 2, 1)
    gains = jnp.concatenate([gain_a, widen(gain_b, 1)], axis=0)
    gain = lax.dynamic_slice_in_dim(gains, mine, 1, 0)
    share = jnp.full((1, 128), jnp.where(mine < heads, 1.0 / width_a, 1.0 / width_b), jnp.float32)
    first_q, first_k = width_a // width_k, width_a // width_k + 1

    def block(width, first):
        return pl.BlockSpec((1, length, width), lambda t: (t, 0, first))

    def every(width, first):
        return pl.BlockSpec((count, length, width), lambda t: (0, 0, first))

    def by_block(*shape):
        return pl.BlockSpec((1,) + shape, lambda t: (t, 0, 0))

    def fixed(*shape):
        return pl.BlockSpec(shape, lambda t: (0, 0))

    out = pl.pallas_call(
        unit_kernel,
        grid=(count,),
        in_specs=[
            block(width_k, first_q),
            block(width_k, first_k),
            block(width_a, 0),
            every(width_k, first_k),
            every(width_a, 0),
            by_block(2, length),
            by_block(2, count * length),
            by_block(length, 2),
            by_block(2, 128),
            fixed(1, width_a),
            fixed(1, 128),
        ],
        out_specs=block(width_a, 0),
        out_shape=jax.ShapeDtypeStruct((count, length, width_a), jnp.bfloat16),
    )(rows, rows, rows, rows, rows, inner, outer, column, peak, gain, share)
    (units,) = exchange([out], 1)

    def lay(parts):
        return jnp.concatenate(parts, axis=1)

    return (
        lay([units[h] for h in range(heads)]),
        lay([units[heads + h][:, :width_b] for h in range(heads)]),
    )


def local(
    query_a,
    key_a,
    value_a,
    query_b,
    key_b,
    value_b,
    in_gate,
    forget_gate,
    head_gain_a,
    head_gain_b,
    out_weight_a,
    out_weight_b,
    residual,
    norm_gain,
    routes,
    route_weights,
    expert_gate,
    expert_up,
    expert_down,
):
    whole_heads = 2 * head_gain_a.shape[0] == lax.axis_size("sp")
    heads_a, heads_b = (mix_units if whole_heads else mix_heads)(
        query_a, key_a, value_a, query_b, key_b, value_b,
        in_gate, forget_gate, head_gain_a, head_gain_b,
    )
    first_term = jnp.einsum("ec,se->cs", out_weight_a, heads_a, preferred_element_type=jnp.float32)
    mix = lax.psum_scatter(
        (
            first_term
            + jnp.einsum("ec,se->cs", out_weight_b, heads_b, preferred_element_type=jnp.float32)
        ).astype(jnp.bfloat16),
        "tp",
        scatter_dimension=0,
        tiled=True,
    ).astype(jnp.float32)
    updated = residual.astype(jnp.float32) + mix
    squares = lax.psum(jnp.sum(updated * updated, axis=0), "tp")
    whole_width = residual.shape[0] * lax.axis_size("tp")
    normed = (
        updated * lax.rsqrt(squares / whole_width + EPSILON)[None, :] * norm_gain[:, None]
    ).astype(jnp.bfloat16)
    token_count = routes.shape[0]
    top_count = routes.shape[1]
    expert_count = lax.axis_size("sp") * expert_gate.shape[0]
    slot_count = 2 * token_count * top_count // expert_count
    flat_routes = routes.reshape(-1)
    hits = (flat_routes[:, None] == jnp.arange(expert_count, dtype=jnp.int32)[None, :]).astype(
        jnp.int32
    )
    ranks = jnp.sum((jnp.cumsum(hits, axis=0) - 1) * hits, axis=1)
    targets = (flat_routes * slot_count + ranks).reshape(token_count, top_count)
    slot_ids = jnp.arange(expert_count * slot_count, dtype=jnp.int32)[:, None]
    selectors = [
        (slot_ids == targets[None, :, ordering_index]).astype(jnp.bfloat16)
        for ordering_index in range(top_count)
    ]
    dispatch = selectors[0]
    ordering_index = 1
    dispatch = dispatch + selectors[ordering_index]
    buffer = jnp.einsum("ps,ds->pd", dispatch, normed, preferred_element_type=jnp.float32)
    buffer = buffer.astype(jnp.bfloat16).reshape(expert_count, slot_count, -1)
    returned = moe(buffer, expert_gate[0], expert_up[0], expert_down[0], 2)
    returned = returned.reshape(-1, returned.shape[-1])
    combined = updated
    for ordering_index in range(top_count):
        picked = jnp.einsum(
            "pd,ps->ds", returned, selectors[ordering_index], preferred_element_type=jnp.float32
        )
        combined = combined + route_weights[:, ordering_index][None, :] * picked
    return combined.astype(jnp.bfloat16)


def solution(mesh):
    placed = (
        P("sp", "tp"),
        P("sp", "tp"),
        P("sp", "tp"),
        P("sp", "tp"),
        P("sp", "tp"),
        P("sp", "tp"),
        P(None, None, "tp", "sp"),
        P(None, None, "tp", "sp"),
        P("tp", None),
        P("tp", None),
        P("tp", None),
        P("tp", None),
        P("tp", "sp"),
        P("tp"),
        P("sp", None),
        P("sp", None),
        P("sp", None, "tp"),
        P("sp", None, "tp"),
        P("sp", "tp", None),
    )
    return jax.shard_map(
        local, mesh=mesh, in_specs=placed, out_specs=P("tp", "sp"), check_vma=False
    )
```

```python
import functools

import jax
import jax.numpy as jnp
from jax import lax
from jax.experimental import pallas as pl
from jax.experimental.pallas import tpu as pltpu
from jax.sharding import PartitionSpec as P

EPSILON = 1e-06
NOTHING = -1e30


def dot(left, right, contract):
    return lax.dot_general(
        left, right, (contract, ((), ())), preferred_element_type=jnp.float32
    )


MESH = pl.DeviceIdType.MESH


def greet(peers):
    barrier = pltpu.get_barrier_semaphore()
    for peer in peers:
        pl.semaphore_signal(barrier, inc=1, device_id=peer, device_id_type=MESH)
    pl.semaphore_wait(barrier, len(peers))


def one_head(query, key, value, keys, values, inner_row, outer_row, column, peak, gain, share):
    length, width_k = query.shape
    scale = width_k ** (-0.5)
    rows = lax.broadcasted_iota(jnp.int32, (length, length), 0)
    lanes = lax.broadcasted_iota(jnp.int32, (length, length), 1)
    near = dot(query, key, ((1,), (1,))) * scale
    far = dot(query, keys, ((1,), (1,))) * scale
    far_scores = [far * outer_row[r] for r in range(2)]
    far_sums = [jnp.sum(scores, axis=1, keepdims=True) for scores in far_scores]
    far_values = dot(
        jnp.concatenate([scores.astype(jnp.bfloat16) for scores in far_scores], axis=0),
        values,
        ((1,), (0,)),
    )
    both = None
    for r in range(2):
        keep = lanes <= rows if r == 0 else lanes >= rows
        logs = jnp.where(keep, column[r] + inner_row[r], NOTHING)
        carried_log = column[r] + peak[r]
        top = jnp.maximum(carried_log, jnp.max(logs, axis=1, keepdims=True))
        carried = jnp.exp(carried_log - top)
        scores = near * jnp.exp(logs - top)
        numer = carried * far_values[r * length : (r + 1) * length] + dot(
            scores.astype(jnp.bfloat16), value, ((1,), (0,))
        )
        denom = carried * far_sums[r] + jnp.sum(scores, axis=1, keepdims=True)
        out = numer / jnp.maximum(jnp.abs(denom), jnp.exp(-top))
        both = out if both is None else both + out
    mean = jnp.sum(both * both, axis=1, keepdims=True) * share
    return (both * lax.rsqrt(mean + EPSILON) * gain).astype(jnp.bfloat16)


def mixer_kernel(
    qa, ka, va, qb, kb, vb, all_ka, all_va, all_kb, all_vb,
    inner, outer, column, peak, gain_a, gain_b, heads_a, heads_b,
):
    parts = (
        (qa, ka, va, all_ka, all_va, gain_a, heads_a),
        (qb, kb, vb, all_kb, all_vb, gain_b, heads_b),
    )
    for g, (q, k, v, every_k, every_v, gain, heads) in enumerate(parts):
        heads[...] = one_head(
            q[...], k[...], v[...], every_k[...], every_v[...],
            [inner[0, 2 * r + g : 2 * r + g + 1, :] for r in range(2)],
            [outer[0, 2 * r + g : 2 * r + g + 1, :] for r in range(2)],
            [column[0, :, 2 * r + g : 2 * r + g + 1] for r in range(2)],
            [peak[0, 2 * r + g : 2 * r + g + 1, 0:1] for r in range(2)],
            gain[0],
            1.0 / gain.shape[-1],
        )


def mix_heads(query_a, key_a, value_a, query_b, key_b, value_b, in_gate, forget_gate, gain_a, gain_b):
    heads = gain_a.shape[0]
    length = query_a.shape[0]
    width_k = query_a.shape[1] // heads
    width_a, width_b = gain_a.shape[1], gain_b.shape[1]
    count, mine = lax.axis_size("sp"), lax.axis_index("sp")
    packed = jnp.concatenate([value_a, key_a, key_b, value_b], axis=1)
    gathered = lax.all_gather(packed, "sp", axis=0, tiled=True)
    total_rows = gathered.shape[0]
    log_decay = jax.nn.log_sigmoid(forget_gate)
    ones = jnp.ones((length, length), jnp.float32)
    exact = lax.Precision.HIGHEST
    run = jnp.stack(
        [
            jnp.einsum("ghs,st->ght", log_decay[0], jnp.triu(ones), precision=exact),
            jnp.einsum("ghs,st->ght", log_decay[1], jnp.tril(ones), precision=exact),
        ]
    )
    whole = jnp.sum(log_decay, axis=-1, keepdims=True)
    tails = in_gate + whole - run
    small = lax.all_gather(
        jnp.stack([tails, jnp.broadcast_to(whole, tails.shape)]), "sp", axis=0
    )
    every_tail, every_whole = small[:, 0], small[:, 1, ..., 0]
    place = jnp.arange(count)
    source, middle = place[:, None], place[None, :]
    between = jnp.stack(
        [
            (middle > source) & (middle < mine),
            (middle < source) & (middle > mine),
        ]
    ).astype(jnp.float32)
    gap = jnp.sum(between[:, :, :, None, None] * jnp.moveaxis(every_whole, 0, 1)[:, None], axis=2)
    seen = jnp.stack([place < mine, place > mine])[:, :, None, None, None]
    logs = jnp.where(seen, jnp.moveaxis(every_tail, 0, 1) + gap[..., None], NOTHING)
    peak = jnp.max(logs, axis=(1, 4))
    outer = jnp.where(seen, jnp.exp(logs - peak[:, None, :, :, None]), 0.0)
    outer = outer.transpose(3, 0, 2, 1, 4).reshape(heads, 4, total_rows)
    peak = jnp.broadcast_to(peak.transpose(2, 0, 1).reshape(heads, 4, 1), (heads, 4, 128))
    inner = (in_gate - run).transpose(2, 0, 1, 3).reshape(heads, 4, length)
    column = run.transpose(2, 3, 0, 1).reshape(heads, length, 4)
    ratio = width_a // width_k

    def columns(rows, width, first):
        return pl.BlockSpec((rows, width), lambda h: (0, first + h))

    def by_head(*shape):
        return pl.BlockSpec((1,) + shape, lambda h: (h, 0, 0))

    return pl.pallas_call(
        mixer_kernel,
        grid=(heads,),
        in_specs=[
            columns(length, width_k, 0),
            columns(length, width_k, 0),
            columns(length, width_a, 0),
            columns(length, width_k, 0),
            columns(length, width_k, 0),
            columns(length, width_b, 0),
            columns(total_rows, width_k, ratio * heads),
            columns(total_rows, width_a, 0),
            columns(total_rows, width_k, (ratio + 1) * heads),
            columns(total_rows, width_b, (ratio + 2) * heads),
            by_head(4, length),
            by_head(4, total_rows),
            by_head(length, 4),
            by_head(4, 128),
            by_head(1, width_a),
            by_head(1, width_b),
        ],
        out_specs=[columns(length, width_a, 0), columns(length, width_b, 0)],
        out_shape=[
            jax.ShapeDtypeStruct((length, heads * width_a), jnp.bfloat16),
            jax.ShapeDtypeStruct((length, heads * width_b), jnp.bfloat16),
        ],
        cost_estimate=pl.CostEstimate(
            flops=4 * heads * length * total_rows * (2 * width_k + 2 * width_a),
            bytes_accessed=2 * packed.size * count,
            transcendentals=0,
        ),
    )(
        query_a, key_a, value_a, query_b, key_b, value_b,
        gathered, gathered, gathered, gathered,
        inner, outer, column, peak, gain_a[:, None, :], gain_b[:, None, :],
    )


EXACT = lax.Precision.HIGHEST


def exact_dot(left, right, contract):
    return lax.dot_general(
        left, right, (contract, ((), ())), precision=EXACT, preferred_element_type=jnp.float32
    )


def flip(index, mask):
    bit, result = 1, index
    while bit <= mask:
        if mask & bit:
            result = result + bit * (1 - 2 * lax.rem(lax.div(index, bit), 2))
        bit = 2 * bit
    return result


def partners(mine, count):
    if count & (count - 1) == 0:
        peers = [flip(mine, step) for step in range(count)]
        return peers, peers
    ahead = [lax.rem(mine + step, count) for step in range(count)]
    return ahead, [lax.rem(mine + count - step, count) for step in range(count)]


def arrival_order(count):
    near, far = list(range(1, count // 2)), list(range(count // 2, count))
    order = [0]
    while near or far:
        if near:
            order.append(near.pop(0))
        if far:
            order.append(far.pop(0))
    return order


class Names:
    pass


def upright(row):
    length = row.shape[1]
    diagonal = lax.broadcasted_iota(jnp.int32, (length, length), 0) == lax.broadcasted_iota(
        jnp.int32, (length, length), 1
    )
    return jnp.sum(jnp.where(diagonal, row, jnp.zeros_like(row)), axis=1, keepdims=True)


def send(source, target, pair, at, device):
    copy = pltpu.make_async_remote_copy(
        src_ref=source, dst_ref=target, send_sem=pair[0].at[at], recv_sem=pair[1].at[at],
        device_id=device, device_id_type=MESH,
    )
    copy.start()
    return copy


def near_sums(near, far, v, values, outer, inner, column, peak, keep):
    far_scores = far * outer
    far_sum = jnp.sum(far_scores, axis=1, keepdims=True)
    far_values = dot(far_scores.astype(jnp.bfloat16), values, ((1,), (0,)))
    logs = jnp.where(keep, column + inner, NOTHING)
    far_log = column + peak
    top = jnp.maximum(far_log, jnp.max(logs, axis=1, keepdims=True))
    far_part = jnp.exp(far_log - top)
    scores = near * jnp.exp(logs - top)
    numer = far_part * far_values + dot(scores.astype(jnp.bfloat16), v, ((1,), (0,)))
    denom = far_part * far_sum + jnp.sum(scores, axis=1, keepdims=True)
    return numer, denom, top


def settle(numer, denom, top):
    return numer / jnp.maximum(jnp.abs(denom), jnp.exp(-top))


def gate_part(n):
    blocks = n.gates.shape[0]
    for r in range(2):
        for g in range(2):
            inputs, forget = n.in_gate[r, g], n.forget_gate[r, g]
            decay = jnp.minimum(forget, 0.0) - jnp.log1p(jnp.exp(-jnp.abs(forget)))
            at = 2 * r + g
            for h in range(blocks):
                n.gates[h, at : at + 1] = inputs[h : h + 1]
                n.gates[h, 4 + at : 5 + at] = decay[h : h + 1]


def mixer_part(n):
    blocks = n.gates.shape[0]
    mine = lax.axis_index("sp")
    part = lax.div(mine, blocks)
    at = lax.rem(mine, blocks)
    length = n.qa.shape[0]
    fields = (
        (n.ka, n.all_ka), (n.va, n.all_va), (n.qa, n.all_qa),
        (n.kb, n.all_kb), (n.vb, n.all_vb), (n.qb, n.all_qb),
    )

    def columns(field, target, head):
        width = target.shape[-1]
        return field.at[:, pl.ds(pl.multiple_of(head * width, width), width)]

    kept = [pltpu.make_async_copy(n.gates.at[at], n.all_gates.at[at], n.m_kept.at[6])]
    for f, (field, target) in enumerate(fields):
        kept.append(pltpu.make_async_copy(columns(field, target, at), target.at[at], n.m_kept.at[f]))
    for copy in kept:
        copy.start()
    went = []
    to, of = partners(at, blocks)
    peers, givers = to[1:], of[1:]
    for step, peer in enumerate(peers):
        went.append(
            send(
                n.gates.at[peer], n.all_gates.at[at], (n.m_sent, n.m_landed), (step, 6),
                {"sp": part * blocks + peer},
            )
        )
    for f, (field, target) in enumerate(fields):
        for step, peer in enumerate(peers):
            went.append(
                send(
                    columns(field, target, peer), target.at[at],
                    (n.m_sent, n.m_landed), (step, f), {"sp": part * blocks + peer},
                )
            )
    near = blocks - 1
    for copy in kept:
        copy.wait()
    for copy in went[:near]:
        copy.wait_recv()
    rows = lax.broadcasted_iota(jnp.int32, (length, length), 0)
    lanes = lax.broadcasted_iota(jnp.int32, (length, length), 1)
    upper = (rows <= lanes).astype(jnp.float32)
    lower = (rows >= lanes).astype(jnp.float32)
    ahead = lax.broadcasted_iota(jnp.int32, (4, 1), 0) < 2
    ahead_lane = lax.broadcasted_iota(jnp.int32, (length, 4), 1) < 2
    tails, wholes = [], []
    for b in range(blocks):
        inputs, decay = n.all_gates[b, 0:4], n.all_gates[b, 4:8]
        run = jnp.where(
            ahead,
            exact_dot(decay, upper, ((1,), (0,))),
            exact_dot(decay, lower, ((1,), (0,))),
        )
        n.column[b] = jnp.where(
            ahead_lane,
            exact_dot(lower, decay, ((1,), (1,))),
            exact_dot(upper, decay, ((1,), (1,))),
        )
        whole = jnp.sum(decay, axis=1, keepdims=True)
        n.inner[b] = inputs - run
        tails.append(inputs + whole - run)
        wholes.append(whole)
    nothing = jnp.zeros((4, 1), jnp.float32)
    before, after = [nothing], [nothing]
    for b in range(blocks - 1):
        before.append(before[-1] + wholes[b])
        after.insert(0, after[0] + wholes[blocks - 1 - b])
    ends = [tails[b] + jnp.where(ahead, after[b], before[b]) for b in range(blocks)]
    peak = functools.reduce(
        jnp.maximum, [jnp.max(logs, axis=1, keepdims=True) for logs in ends]
    )
    first = part == 0
    weights = [jnp.exp(logs - peak) for logs in ends]
    weights = [jnp.where(first, w[0:2], w[2:4]) for w in weights]
    n.note[2:4] = jnp.broadcast_to(jnp.where(first, peak[0:2], peak[2:4]), (2, length))
    for t in range(blocks):
        seen = []
        for b in range(blocks):
            if b < t:
                logs = tails[b] + sum(wholes[b + 1 : t], nothing)
                seen.append(jnp.where(ahead, logs, NOTHING))
            elif b > t:
                logs = tails[b] + sum(wholes[t + 1 : b], nothing)
                seen.append(jnp.where(ahead, NOTHING, logs))
            else:
                seen.append(jnp.full((4, length), NOTHING, jnp.float32))
        top = functools.reduce(
            jnp.maximum, [jnp.max(logs, axis=1, keepdims=True) for logs in seen]
        )
        for b in range(blocks):
            n.outer[t, :, b * length : (b + 1) * length] = jnp.where(
                seen[b] > 0.5 * NOTHING, jnp.exp(seen[b] - top), 0.0
            )
        n.peak[t] = jnp.broadcast_to(top, (4, length))
        n.offset[t] = jnp.broadcast_to(jnp.where(ahead, before[t], after[t]), (4, length))
    other = {"sp": lax.rem(mine + blocks, 2 * blocks)}
    n.note[4:8] = jnp.zeros((4, length), jnp.float32)
    states = []

    def landed(*waves):
        for wave in waves:
            for copy in went[(1 + wave) * near : (2 + wave) * near]:
                copy.wait_recv()

    def state(g):
        keys, values, memory, far = (
            (n.all_ka, n.all_va, n.memory_a, n.far_a), (n.all_kb, n.all_vb, n.memory_b, n.far_b)
        )[g]
        total, normal = None, None
        for b in range(blocks):
            key = keys[b].astype(jnp.float32).T * weights[b][g : g + 1]
            piece = dot(key.astype(jnp.bfloat16), values[b], ((1,), (0,)))
            total = piece if total is None else total + piece
            amount = exact_dot(weights[b], keys[b].astype(jnp.float32), ((1,), (0,)))[g : g + 1]
            normal = amount if normal is None else normal + amount
        memory[...] = total.astype(jnp.bfloat16)
        n.note[g : g + 1] = normal
        states.append(send(memory, far, (n.h_sent, n.h_landed), g, other))

    def local_pass(g, start, stop):
        q, k, v, shut, wide = (
            (n.all_qa, n.all_ka, n.all_va, n.shut_a, n.open_a),
            (n.all_qb, n.all_kb, n.all_vb, n.shut_b, n.open_b),
        )[g]
        scale = q.shape[-1] ** (-0.5)
        order = jnp.where(first, 1, -1)
        keeps = [(rows - lanes) * order >= 0, (lanes - rows) * order >= 0]

        @pl.loop(start, stop)
        def _(turn):
            t = lax.rem(at + 1 + turn, blocks)
            keys = k[...].reshape(blocks * length, k.shape[-1])
            values = v[...].reshape(blocks * length, v.shape[-1])
            near_scores = dot(q[t], k[t], ((1,), (1,))) * scale
            far_scores = dot(q[t], keys, ((1,), (1,))) * scale

            def pick(ref, i):
                ahead_row, behind_row = ref[t, g : g + 1], ref[t, 2 + g : 3 + g]
                if i == 0:
                    return jnp.where(first, ahead_row, behind_row)
                return jnp.where(first, behind_row, ahead_row)

            sums = []
            for i in range(2):
                forth, back = n.column[t, :, g : g + 1], n.column[t, :, 2 + g : 3 + g]
                column = jnp.where(first, forth, back) if i == 0 else jnp.where(first, back, forth)
                sums.append(
                    near_sums(
                        near_scores, far_scores, v[t], values, pick(n.outer, i),
                        pick(n.inner, i), column, pick(n.peak, i)[:, 0:1], keeps[i],
                    )
                )
            shut[t] = settle(*sums[0])
            wide[t] = sums[1][0]
            n.stat[t, :, 2 * g : 2 * g + 1] = sums[1][1]
            n.stat[t, :, 2 * g + 1 : 2 * g + 2] = sums[1][2]

    landed(0, 1)
    state(0)
    landed(2)
    local_pass(0, 0, blocks // 2)
    landed(3, 4)
    state(1)
    states.append(send(n.note, n.far_note, (n.h_sent, n.h_landed), 2, other))
    local_pass(0, blocks // 2, blocks)
    landed(5)
    local_pass(1, 0, blocks)
    for copy in states:
        copy.wait_recv()

    def give(t, g):
        source = (n.out_a, n.out_b)[g]
        target = (n.heads_a, n.heads_b)[g]
        width = source.shape[-1]
        return pltpu.make_async_remote_copy(
            src_ref=source.at[t],
            dst_ref=target.at[:, pl.ds(pl.multiple_of(at * width, width), width)],
            send_sem=n.o_sent.at[t, g],
            recv_sem=n.o_landed.at[at, g],
            device_id={"sp": part * blocks + t},
            device_id_type=MESH,
        )

    def keep(g):
        source = (n.out_a, n.out_b)[g]
        target = (n.heads_a, n.heads_b)[g]
        width = source.shape[-1]
        return pltpu.make_async_copy(
            source.at[at],
            target.at[:, pl.ds(pl.multiple_of(at * width, width), width)],
            n.m_kept.at[7 + g],
        )

    @pl.loop(0, blocks)
    def _(turn):
        t = lax.rem(at + 1 + turn, blocks)
        groups = (
            (n.all_qa, n.far_a, n.gain_a, n.shut_a, n.open_a, n.out_a),
            (n.all_qb, n.far_b, n.gain_b, n.shut_b, n.open_b, n.out_b),
        )
        for g, (q, far, gain, shut, wide, out) in enumerate(groups):
            scale = q.shape[-1] ** (-0.5)
            query = q[t]
            reach = dot(query, far[...], ((1,), (0,))) * scale
            reach_sum = (
                jnp.sum(query.astype(jnp.float32) * n.far_note[g : g + 1], axis=1, keepdims=True)
                * scale
            )
            column = jnp.where(first, n.column[t, :, 2 + g : 3 + g], n.column[t, :, g : g + 1])
            offset = jnp.where(
                first, n.offset[t, 2 + g : 3 + g, 0:1], n.offset[t, g : g + 1, 0:1]
            )
            log = column + offset + n.far_note[2 + g : 3 + g, 0:1]
            denom = n.stat[t, :, 2 * g : 2 * g + 1]
            old = n.stat[t, :, 2 * g + 1 : 2 * g + 2]
            top = jnp.maximum(old, log)
            kept_part, reach_part = jnp.exp(old - top), jnp.exp(log - top)
            both = shut[t] + settle(
                kept_part * wide[t] + reach_part * reach,
                kept_part * denom + reach_part * reach_sum,
                top,
            )
            mean = jnp.mean(both * both, axis=1, keepdims=True)
            out[t] = (
                both * lax.rsqrt(mean + EPSILON) * gain[pl.ds(at, 1), :]
            ).astype(jnp.bfloat16)

            @pl.when(t != at)
            def _():
                give(t, g).start()

    def finish():
        for copy in went:
            copy.wait_send()
        for copy in states:
            copy.wait_send()
        for peer in peers:
            for g in range(2):
                give(peer, g).wait_send()

    for g in range(2):
        keep(g).start()
    for g in range(2):
        keep(g).wait()
    for peer in givers:
        for g in range(2):
            width = (n.out_a, n.out_b)[g].shape[-1]
            pltpu.make_async_remote_copy(
                src_ref=(n.out_a, n.out_b)[g].at[at],
                dst_ref=(n.heads_a, n.heads_b)[g].at[
                    :, pl.ds(pl.multiple_of(peer * width, width), width)
                ],
                send_sem=n.o_sent.at[at, g],
                recv_sem=n.o_landed.at[peer, g],
                device_id={"sp": part * blocks + peer},
                device_id_type=MESH,
            ).wait_recv()
    return finish


def project_part(n, count, across):
    slot = lax.axis_index("tp")
    chips = across // 2
    core, row = lax.rem(slot, 2), lax.div(slot, 2)
    twin = slot + 1 - 2 * core
    width = n.residual.shape[0]
    tokens = n.residual.shape[1]
    slots = n.given.shape[1]
    for copy in n.out_weights:
        copy.wait()

    def block(owner):
        columns = pl.ds(pl.multiple_of(owner * width, width), width)
        return dot(n.heads_a[...], n.wa[:, columns], ((1,), (0,))) + dot(
            n.heads_b[...], n.wb[:, columns], ((1,), (0,))
        )

    to_twin, over = [], []
    for turn in range(chips):
        y = lax.rem(row + turn + 1, chips)
        n.mix_out[turn] = block(2 * y + 1 - core).astype(jnp.bfloat16)
        to_twin.append(
            send(n.mix_out.at[turn], n.mix_in.at[turn], (n.p_sent, n.p_landed), turn, {"tp": twin})
        )
        n.mix_own[turn] = block(2 * y + core)
    for turn in range(chips - 1):
        to_twin[turn].wait_recv()
        n.mix_chip[turn] = (n.mix_own[turn] + n.mix_in[turn].astype(jnp.float32)).astype(
            jnp.bfloat16
        )
        other = lax.rem(slot + 2 * (turn + 1), across)
        over.append(
            send(n.mix_chip.at[turn], n.mix_far.at[turn], (n.q_sent, n.q_landed), turn, {"tp": other})
        )
    experts = lax.broadcasted_iota(jnp.int32, (tokens, 128), 1)
    named = [upright(n.routes[k : k + 1, :]) for k in range(n.routes.shape[0])]
    hits = functools.reduce(jnp.logical_or, [experts == e for e in named])
    earlier = lax.broadcasted_iota(jnp.int32, (tokens, tokens), 0) > lax.broadcasted_iota(
        jnp.int32, (tokens, tokens), 1
    )
    ranks = dot(
        earlier.astype(jnp.float32).astype(jnp.bfloat16),
        hits.astype(jnp.float32).astype(jnp.bfloat16),
        ((1,), (0,)),
    )
    places = lax.broadcasted_iota(jnp.int32, (tokens, count * slots), 1).astype(jnp.float32)
    for k, e in enumerate(named):
        target = jnp.sum(
            jnp.where(experts == e, ranks, 0.0), axis=1, keepdims=True
        ) + e.astype(jnp.float32) * slots
        n.choice[k] = (places == target).astype(jnp.float32).astype(jnp.bfloat16)
    picks = functools.reduce(
        jnp.add, [n.choice[k].astype(jnp.float32) for k in range(len(named))]
    )
    picks = picks.T.astype(jnp.bfloat16)
    base = n.residual[...].astype(jnp.float32).T
    to_twin[chips - 1].wait_recv()
    base = base + (n.mix_own[chips - 1] + n.mix_in[chips - 1].astype(jnp.float32))
    for turn in range(chips - 1):
        over[turn].wait_recv()
        base = base + n.mix_far[turn].astype(jnp.float32)
    n.updated[...] = base
    n.squares[0] = exact_dot(jnp.ones((8, width), jnp.float32), base * base, ((1,), (1,)))
    told = []
    for step in range(1, across):
        told.append(
            send(
                n.squares.at[0], n.squares.at[step], (n.v_sent, n.v_landed), step - 1,
                {"tp": lax.rem(slot + step, across)},
            )
        )
    for copy in told:
        copy.wait_recv()
    squares = n.squares[0]
    for step in range(1, across):
        squares = squares + n.squares[step]
    factor = lax.rsqrt(squares[0:1] / (width * across) + EPSILON)
    factor = upright(factor)
    normed = (n.updated[...] * factor * n.norm_gain[...]).astype(jnp.bfloat16)
    n.given[...] = (
        dot(picks, normed, ((1,), (0,))).astype(jnp.bfloat16).reshape(count, slots, width)
    )

    def finish():
        for copy in to_twin + over + told:
            copy.wait_send()

    return finish


def moe_part(n, count, across):
    mine, slot = lax.axis_index("sp"), lax.axis_index("tp")
    chips = across // 2
    given, rows, hidden, part = n.given, n.rows, n.hidden, n.part
    partner, chip, cross, total, out = n.partner, n.chip, n.cross, n.total, n.returned
    slots, width = given.shape[1], given.shape[2]
    units = n.gate_w.shape[1]
    core = lax.rem(slot, 2)
    row = lax.div(slot, 2)
    twin = slot + 1 - 2 * core
    others = [lax.rem(slot + 2 * step, across) for step in range(1, chips)]
    behind = [lax.rem(slot + across - 2 * step, across) for step in range(1, chips)]
    targets, sources = partners(mine, count)
    order = arrival_order(count)

    def place(step, owner):
        return rows.at[step, :, pl.ds(pl.multiple_of(owner * width, width), width)]

    first = [pltpu.make_async_copy(given.at[mine], place(0, slot), n.kept.at[0])]
    first[0].start()
    first += [None] * (count - 1)
    for step in order[1:]:
        first[step] = send(
            given.at[targets[step]], place(order.index(step), slot), (n.sent, n.landed), step,
            {"sp": targets[step]},
        )
    along, last = {}, {}

    def relay(i):
        if i == 0:
            first[0].wait()
        else:
            first[order[i]].wait_recv()
        along[i] = [
            send(place(i, slot), place(i, slot), (n.y_sent, n.y_landed), (i, turn), {"tp": other})
            for turn, other in enumerate(others)
        ]
        last[i] = [
            send(place(i, slot), place(i, slot), (n.c_sent, n.c_landed), (i, 0), {"tp": twin})
        ]

    def hand_over(i):
        for turn, owner in enumerate(behind):
            along[i][turn].wait_recv()
            last[i].append(
                send(
                    place(i, owner), place(i, owner), (n.c_sent, n.c_landed),
                    (i, turn + 1), {"tp": twin},
                )
            )

    groups = 4
    span = count // groups
    tile = min(256, units)
    batch = span * slots
    over, crossed, back = {}, {}, {}

    def block(h):
        return pl.ds(h * span, span)

    def arrive(h):
        for i in range(h * span, (h + 1) * span):
            for copy in last[i]:
                copy.wait_recv()

    def lift(h):
        x = rows[h * span : (h + 1) * span].reshape(batch, width * across)
        for turn in range(units // tile):
            columns = slice(turn * tile, (turn + 1) * tile)
            gate = dot(x, n.gate_w[:, columns], ((1,), (0,)))
            upward = dot(x, n.up_w[:, columns], ((1,), (0,)))
            hidden[h * batch : (h + 1) * batch, columns] = (
                jax.nn.silu(gate) * upward
            ).astype(jnp.bfloat16)

    def lower(h):
        x = hidden[h * batch : (h + 1) * batch, :]
        ys = [lax.rem(row + turn + 1, chips) for turn in range(chips)]
        for whose in (1 - core, core):
            for turn, y in enumerate(ys):
                owner = 2 * y + whose
                columns = pl.ds(pl.multiple_of(owner * width, width), width)
                value = dot(x, n.down_w[:, columns], ((1,), (0,)))
                side = 0 if whose is not core else 1
                part[side, turn, block(h)] = value.astype(jnp.bfloat16).reshape(
                    span, slots, width
                )
                if side == 0:
                    over[h, turn] = send(
                        part.at[0, turn, block(h)], partner.at[turn, block(h)],
                        (n.t_sent, n.t_landed), (h, turn), {"tp": twin},
                    )

    def joined(h, turn):
        over[h, turn].wait_recv()
        return part[1, turn, block(h)].astype(jnp.float32) + partner[turn, block(h)].astype(
            jnp.float32
        )

    def join_twin(h):
        for turn in range(chips - 1):
            chip[turn, block(h)] = joined(h, turn).astype(jnp.bfloat16)
            crossed[h, turn] = send(
                chip.at[turn, block(h)], cross.at[turn, block(h)], (n.r_sent, n.r_landed),
                (h, turn), {"tp": others[turn]},
            )

    def give_back(h):
        value = joined(h, chips - 1)
        for turn in range(chips - 1):
            crossed[h, turn].wait_recv()
            value = value + cross[turn, block(h)].astype(jnp.float32)
        total[block(h)] = value.astype(jnp.bfloat16)
        for i in range(h * span, (h + 1) * span):
            step = order[i]
            if step == 0:
                back[step] = pltpu.make_async_copy(total.at[i], out.at[mine], n.kept.at[1])
                back[step].start()
            else:
                back[step] = send(
                    total.at[i], out.at[mine], (n.s_sent, n.s_landed), step,
                    {"sp": sources[step]},
                )

    def weights_in(picked):
        for copy in picked:
            copy.wait()

    tasks = {
        2 * span: [
            functools.partial(weights_in, n.expert_weights[:2]),
            functools.partial(arrive, 0), functools.partial(lift, 0),
        ],
        2 * span + 1: [
            functools.partial(weights_in, n.expert_weights[2:]), functools.partial(lower, 0),
        ],
        3 * span: [
            functools.partial(arrive, 1), functools.partial(lift, 1),
            functools.partial(join_twin, 0), functools.partial(lower, 1),
        ],
    }
    relay(0)
    for i in range(1, count):
        for task in tasks.get(i, []):
            task()
        relay(i)
        hand_over(i - 1)
    hand_over(count - 1)
    arrive(2)
    lift(2)
    join_twin(1)
    lower(2)
    give_back(0)
    arrive(3)
    join_twin(2)
    lift(3)
    lower(3)
    give_back(1)
    join_twin(3)
    give_back(2)
    give_back(3)
    back[0].wait()
    for i in range(count):
        if i > 0:
            first[i].wait_send()
            back[i].wait()
        for copy in along[i] + last[i]:
            copy.wait_send()
    for copy in list(over.values()) + list(crossed.values()):
        copy.wait_send()


def layer_kernel(count, across, names, mixing, *refs):
    n = Names()
    for name, ref in zip(names, refs):
        setattr(n, name, ref)
    mine, slot = lax.axis_index("sp"), lax.axis_index("tp")
    n.out_weights = [
        pltpu.make_async_copy(source, target, n.weight.at[i])
        for i, (source, target) in enumerate(((n.out_wa, n.wa), (n.out_wb, n.wb)))
    ]
    n.expert_weights = [
        pltpu.make_async_copy(source, target, n.weight.at[2 + i])
        for i, (source, target) in enumerate(
            ((n.gate, n.gate_w), (n.up, n.up_w), (n.down, n.down_w))
        )
    ]
    peers = [{"sp": lax.rem(mine + step, count)} for step in range(1, count)]
    peers += [{"tp": lax.rem(slot + step, across)} for step in range(1, across)]
    barrier = pltpu.get_barrier_semaphore()
    for peer in peers:
        pl.semaphore_signal(barrier, inc=1, device_id=peer, device_id_type=MESH)
    for copy in n.out_weights + n.expert_weights:
        copy.start()
    if mixing:
        gate_part(n)
    pl.semaphore_wait(barrier, len(peers))
    done = []
    if mixing:
        done.append(mixer_part(n))
    done.append(project_part(n, count, across))
    moe_part(n, count, across)
    result = n.updated[...]
    returned = n.returned[...].reshape(-1, n.returned.shape[-1])
    for k in range(n.choice.shape[0]):
        result = result + upright(n.route_weights[k : k + 1, :]) * dot(
            n.choice[k], returned, ((1,), (0,))
        )
    n.out[...] = result.T.astype(jnp.bfloat16)
    for finish in done:
        finish()


def layer(mixer, others, weights, count, across, slots, number):
    bf16, f32 = jnp.bfloat16, jnp.float32
    vmem = pl.BlockSpec(memory_space=pltpu.VMEM)
    whole = pl.BlockSpec(memory_space=pl.ANY)
    dma = pltpu.SemaphoreType.DMA
    chips = across // 2
    width, tokens = others["residual"].shape
    top = others["routes"].shape[0]
    units = weights["gate"].shape[1]
    mixing = "qa" in mixer
    pieces = 4
    scratch = {}

    def buffer(name, shape, dtype=bf16):
        scratch[name] = pltpu.VMEM(shape, dtype)

    def pair(name, shape):
        scratch[name + "_sent"] = dma(shape)
        scratch[name + "_landed"] = dma(shape)

    if mixing:
        blocks = mixer["gain_a"].shape[0]
        wide_a, wide_b = mixer["gain_a"].shape[1], mixer["gain_b"].shape[1]
        dk = mixer["qa"].shape[1] // blocks
        for g, wide in (("a", wide_a), ("b", wide_b)):
            buffer("all_q" + g, (blocks, tokens, dk))
            buffer("all_k" + g, (blocks, tokens, dk))
            buffer("all_v" + g, (blocks, tokens, wide))
            buffer("memory_" + g, (dk, wide))
            buffer("far_" + g, (dk, wide))
            buffer("out_" + g, (blocks, tokens, wide))
            buffer("shut_" + g, (blocks, tokens, wide), f32)
            buffer("open_" + g, (blocks, tokens, wide), f32)
            buffer("heads_" + g, (tokens, blocks * wide))
        buffer("gates", (blocks, 8, tokens), f32)
        buffer("all_gates", (blocks, 8, tokens), f32)
        buffer("note", (8, tokens), f32)
        buffer("far_note", (8, tokens), f32)
        buffer("column", (blocks, tokens, 4), f32)
        buffer("stat", (blocks, tokens, 4), f32)
        buffer("inner", (blocks, 4, tokens), f32)
        buffer("outer", (blocks, 4, blocks * tokens), f32)
        buffer("peak", (blocks, 4, tokens), f32)
        buffer("offset", (blocks, 4, tokens), f32)
        scratch["m_kept"] = dma((9,))
        pair("m", (blocks - 1, 7))
        pair("h", (3,))
        pair("o", (blocks, 2))
    buffer("wa", weights["out_wa"].shape)
    buffer("wb", weights["out_wb"].shape)
    buffer("mix_out", (chips, tokens, width))
    buffer("mix_in", (chips, tokens, width))
    buffer("mix_own", (chips, tokens, width), f32)
    buffer("mix_chip", (chips - 1, tokens, width))
    buffer("mix_far", (chips - 1, tokens, width))
    buffer("updated", (tokens, width), f32)
    buffer("squares", (across, 8, tokens), f32)
    buffer("choice", (top, tokens, count * slots))
    buffer("given", (count, slots, width))
    buffer("returned", (count, slots, width))
    buffer("rows", (count, slots, width * across))
    buffer("gate_w", weights["gate"].shape)
    buffer("up_w", weights["up"].shape)
    buffer("down_w", weights["down"].shape)
    buffer("hidden", (count * slots, units))
    buffer("part", (2, chips, count, slots, width))
    buffer("partner", (chips, count, slots, width))
    buffer("chip", (chips - 1, count, slots, width))
    buffer("cross", (chips - 1, count, slots, width))
    buffer("total", (count, slots, width))
    scratch["kept"] = dma((2,))
    scratch["weight"] = dma((5,))
    pair("p", (chips,))
    pair("q", (chips - 1,))
    pair("v", (across - 1,))
    scratch["sent"], scratch["landed"] = dma((count,)), dma((count,))
    pair("y", (count, chips - 1))
    pair("c", (count, chips))
    pair("t", (pieces, chips))
    pair("r", (pieces, chips - 1))
    pair("s", (count,))
    inputs = {**mixer, **others, **weights}
    names = list(inputs) + ["out"] + list(scratch)
    return pl.pallas_call(
        functools.partial(layer_kernel, count, across, names, mixing),
        out_shape=jax.ShapeDtypeStruct((width, tokens), bf16),
        in_specs=[whole if name in weights else vmem for name in inputs],
        out_specs=vmem,
        scratch_shapes=list(scratch.values()),
        compiler_params=pltpu.CompilerParams(
            collective_id=number, has_side_effects=True, vmem_limit_bytes=56 * 1024 * 1024
        ),
    )(*inputs.values())


def local(
    query_a,
    key_a,
    value_a,
    query_b,
    key_b,
    value_b,
    in_gate,
    forget_gate,
    head_gain_a,
    head_gain_b,
    out_weight_a,
    out_weight_b,
    residual,
    norm_gain,
    routes,
    route_weights,
    expert_gate,
    expert_up,
    expert_down,
):
    count, across = lax.axis_size("sp"), lax.axis_size("tp")
    heads = head_gain_a.shape[0]
    if 2 * heads == count:
        mixer = dict(
            qa=query_a, ka=key_a, va=value_a, qb=query_b, kb=key_b, vb=value_b,
            in_gate=in_gate, forget_gate=forget_gate, gain_a=head_gain_a, gain_b=head_gain_b,
        )
    else:
        heads_a, heads_b = mix_heads(
            query_a, key_a, value_a, query_b, key_b, value_b,
            in_gate, forget_gate, head_gain_a, head_gain_b,
        )
        mixer = dict(heads_a=heads_a, heads_b=heads_b)
    token_count, top_count = routes.shape
    expert_count = count * expert_gate.shape[0]
    slots = 2 * token_count * top_count // expert_count
    others = dict(
        residual=residual, norm_gain=norm_gain[None, :], routes=routes.T,
        route_weights=route_weights.T,
    )
    weights = dict(
        out_wa=out_weight_a, out_wb=out_weight_b,
        gate=expert_gate[0], up=expert_up[0], down=expert_down[0],
    )
    return layer(mixer, others, weights, count, across, slots, 0)


def solution(mesh):
    placed = (
        P("sp", "tp"),
        P("sp", "tp"),
        P("sp", "tp"),
        P("sp", "tp"),
        P("sp", "tp"),
        P("sp", "tp"),
        P(None, None, "tp", "sp"),
        P(None, None, "tp", "sp"),
        P("tp", None),
        P("tp", None),
        P("tp", None),
        P("tp", None),
        P("tp", "sp"),
        P("tp"),
        P("sp", None),
        P("sp", None),
        P("sp", None, "tp"),
        P("sp", None, "tp"),
        P("sp", "tp", None),
    )
    return jax.shard_map(
        local, mesh=mesh, in_specs=placed, out_specs=P("tp", "sp"), check_vma=False
    )
```

```python
import functools

import jax
import jax.numpy as jnp
from jax import lax
from jax.experimental import pallas as pl
from jax.experimental.pallas import tpu as pltpu
from jax.sharding import PartitionSpec as P

EPSILON = 1e-06
NOTHING = -1e30


def dot(left, right, contract):
    return lax.dot_general(
        left, right, (contract, ((), ())), preferred_element_type=jnp.float32
    )


MESH = pl.DeviceIdType.MESH


def greet(peers):
    barrier = pltpu.get_barrier_semaphore()
    for peer in peers:
        pl.semaphore_signal(barrier, inc=1, device_id=peer, device_id_type=MESH)
    pl.semaphore_wait(barrier, len(peers))


def one_head(query, key, value, keys, values, inner_row, outer_row, column, peak, gain, share):
    length, width_k = query.shape
    scale = width_k ** (-0.5)
    rows = lax.broadcasted_iota(jnp.int32, (length, length), 0)
    lanes = lax.broadcasted_iota(jnp.int32, (length, length), 1)
    near = dot(query, key, ((1,), (1,))) * scale
    far = dot(query, keys, ((1,), (1,))) * scale
    far_scores = [far * outer_row[r] for r in range(2)]
    far_sums = [jnp.sum(scores, axis=1, keepdims=True) for scores in far_scores]
    far_values = dot(
        jnp.concatenate([scores.astype(jnp.bfloat16) for scores in far_scores], axis=0),
        values,
        ((1,), (0,)),
    )
    both = None
    for r in range(2):
        keep = lanes <= rows if r == 0 else lanes >= rows
        logs = jnp.where(keep, column[r] + inner_row[r], NOTHING)
        carried_log = column[r] + peak[r]
        top = jnp.maximum(carried_log, jnp.max(logs, axis=1, keepdims=True))
        carried = jnp.exp(carried_log - top)
        scores = near * jnp.exp(logs - top)
        numer = carried * far_values[r * length : (r + 1) * length] + dot(
            scores.astype(jnp.bfloat16), value, ((1,), (0,))
        )
        denom = carried * far_sums[r] + jnp.sum(scores, axis=1, keepdims=True)
        out = numer / jnp.maximum(jnp.abs(denom), jnp.exp(-top))
        both = out if both is None else both + out
    mean = jnp.sum(both * both, axis=1, keepdims=True) * share
    return (both * lax.rsqrt(mean + EPSILON) * gain).astype(jnp.bfloat16)


def mixer_kernel(
    qa, ka, va, qb, kb, vb, all_ka, all_va, all_kb, all_vb,
    inner, outer, column, peak, gain_a, gain_b, heads_a, heads_b,
):
    parts = (
        (qa, ka, va, all_ka, all_va, gain_a, heads_a),
        (qb, kb, vb, all_kb, all_vb, gain_b, heads_b),
    )
    for g, (q, k, v, every_k, every_v, gain, heads) in enumerate(parts):
        heads[...] = one_head(
            q[...], k[...], v[...], every_k[...], every_v[...],
            [inner[0, 2 * r + g : 2 * r + g + 1, :] for r in range(2)],
            [outer[0, 2 * r + g : 2 * r + g + 1, :] for r in range(2)],
            [column[0, :, 2 * r + g : 2 * r + g + 1] for r in range(2)],
            [peak[0, 2 * r + g : 2 * r + g + 1, 0:1] for r in range(2)],
            gain[0],
            1.0 / gain.shape[-1],
        )


def mix_heads(query_a, key_a, value_a, query_b, key_b, value_b, in_gate, forget_gate, gain_a, gain_b):
    heads = gain_a.shape[0]
    length = query_a.shape[0]
    width_k = query_a.shape[1] // heads
    width_a, width_b = gain_a.shape[1], gain_b.shape[1]
    count, mine = lax.axis_size("sp"), lax.axis_index("sp")
    packed = jnp.concatenate([value_a, key_a, key_b, value_b], axis=1)
    gathered = lax.all_gather(packed, "sp", axis=0, tiled=True)
    total_rows = gathered.shape[0]
    log_decay = jax.nn.log_sigmoid(forget_gate)
    ones = jnp.ones((length, length), jnp.float32)
    exact = lax.Precision.HIGHEST
    run = jnp.stack(
        [
            jnp.einsum("ghs,st->ght", log_decay[0], jnp.triu(ones), precision=exact),
            jnp.einsum("ghs,st->ght", log_decay[1], jnp.tril(ones), precision=exact),
        ]
    )
    whole = jnp.sum(log_decay, axis=-1, keepdims=True)
    tails = in_gate + whole - run
    small = lax.all_gather(
        jnp.stack([tails, jnp.broadcast_to(whole, tails.shape)]), "sp", axis=0
    )
    every_tail, every_whole = small[:, 0], small[:, 1, ..., 0]
    place = jnp.arange(count)
    source, middle = place[:, None], place[None, :]
    between = jnp.stack(
        [
            (middle > source) & (middle < mine),
            (middle < source) & (middle > mine),
        ]
    ).astype(jnp.float32)
    gap = jnp.sum(between[:, :, :, None, None] * jnp.moveaxis(every_whole, 0, 1)[:, None], axis=2)
    seen = jnp.stack([place < mine, place > mine])[:, :, None, None, None]
    logs = jnp.where(seen, jnp.moveaxis(every_tail, 0, 1) + gap[..., None], NOTHING)
    peak = jnp.max(logs, axis=(1, 4))
    outer = jnp.where(seen, jnp.exp(logs - peak[:, None, :, :, None]), 0.0)
    outer = outer.transpose(3, 0, 2, 1, 4).reshape(heads, 4, total_rows)
    peak = jnp.broadcast_to(peak.transpose(2, 0, 1).reshape(heads, 4, 1), (heads, 4, 128))
    inner = (in_gate - run).transpose(2, 0, 1, 3).reshape(heads, 4, length)
    column = run.transpose(2, 3, 0, 1).reshape(heads, length, 4)
    ratio = width_a // width_k

    def columns(rows, width, first):
        return pl.BlockSpec((rows, width), lambda h: (0, first + h))

    def by_head(*shape):
        return pl.BlockSpec((1,) + shape, lambda h: (h, 0, 0))

    return pl.pallas_call(
        mixer_kernel,
        grid=(heads,),
        in_specs=[
            columns(length, width_k, 0),
            columns(length, width_k, 0),
            columns(length, width_a, 0),
            columns(length, width_k, 0),
            columns(length, width_k, 0),
            columns(length, width_b, 0),
            columns(total_rows, width_k, ratio * heads),
            columns(total_rows, width_a, 0),
            columns(total_rows, width_k, (ratio + 1) * heads),
            columns(total_rows, width_b, (ratio + 2) * heads),
            by_head(4, length),
            by_head(4, total_rows),
            by_head(length, 4),
            by_head(4, 128),
            by_head(1, width_a),
            by_head(1, width_b),
        ],
        out_specs=[columns(length, width_a, 0), columns(length, width_b, 0)],
        out_shape=[
            jax.ShapeDtypeStruct((length, heads * width_a), jnp.bfloat16),
            jax.ShapeDtypeStruct((length, heads * width_b), jnp.bfloat16),
        ],
        cost_estimate=pl.CostEstimate(
            flops=4 * heads * length * total_rows * (2 * width_k + 2 * width_a),
            bytes_accessed=2 * packed.size * count,
            transcendentals=0,
        ),
    )(
        query_a, key_a, value_a, query_b, key_b, value_b,
        gathered, gathered, gathered, gathered,
        inner, outer, column, peak, gain_a[:, None, :], gain_b[:, None, :],
    )


EXACT = lax.Precision.HIGHEST


def exact_dot(left, right, contract):
    return lax.dot_general(
        left, right, (contract, ((), ())), precision=EXACT, preferred_element_type=jnp.float32
    )


def flip(index, mask):
    bit, result = 1, index
    while bit <= mask:
        if mask & bit:
            result = result + bit * (1 - 2 * lax.rem(lax.div(index, bit), 2))
        bit = 2 * bit
    return result


def partners(mine, count):
    if count & (count - 1) == 0:
        peers = [flip(mine, step) for step in range(count)]
        return peers, peers
    ahead = [lax.rem(mine + step, count) for step in range(count)]
    return ahead, [lax.rem(mine + count - step, count) for step in range(count)]


def arrival_order(count):
    near, far = list(range(1, count // 2)), list(range(count // 2, count))
    order = [0]
    while near or far:
        if near:
            order.append(near.pop(0))
        if far:
            order.append(far.pop(0))
    return order


class Names:
    pass


def upright(row):
    length = row.shape[1]
    diagonal = lax.broadcasted_iota(jnp.int32, (length, length), 0) == lax.broadcasted_iota(
        jnp.int32, (length, length), 1
    )
    return jnp.sum(jnp.where(diagonal, row, jnp.zeros_like(row)), axis=1, keepdims=True)


def send(source, target, pair, at, device):
    copy = pltpu.make_async_remote_copy(
        src_ref=source, dst_ref=target, send_sem=pair[0].at[at], recv_sem=pair[1].at[at],
        device_id=device, device_id_type=MESH,
    )
    copy.start()
    return copy


def near_sums(near, far, v, values, outer, inner, column, peak, keep):
    far_scores = far * outer
    far_sum = jnp.sum(far_scores, axis=1, keepdims=True)
    far_values = dot(far_scores.astype(jnp.bfloat16), values, ((1,), (0,)))
    logs = jnp.where(keep, column + inner, NOTHING)
    far_log = column + peak
    top = jnp.maximum(far_log, jnp.max(logs, axis=1, keepdims=True))
    far_part = jnp.exp(far_log - top)
    scores = near * jnp.exp(logs - top)
    numer = far_part * far_values + dot(scores.astype(jnp.bfloat16), v, ((1,), (0,)))
    denom = far_part * far_sum + jnp.sum(scores, axis=1, keepdims=True)
    return numer, denom, top


def settle(numer, denom, top):
    return numer / jnp.maximum(jnp.abs(denom), jnp.exp(-top))


def gate_part(n):
    blocks = n.gates.shape[0]
    for r in range(2):
        for g in range(2):
            inputs, forget = n.in_gate[r, g], n.forget_gate[r, g]
            decay = jnp.minimum(forget, 0.0) - jnp.log1p(jnp.exp(-jnp.abs(forget)))
            at = 2 * r + g
            for h in range(blocks):
                n.gates[h, at : at + 1] = inputs[h : h + 1]
                n.gates[h, 4 + at : 5 + at] = decay[h : h + 1]


def mixer_part(n):
    blocks = n.gates.shape[0]
    mine = lax.axis_index("sp")
    part = lax.div(mine, blocks)
    at = lax.rem(mine, blocks)
    length = n.qa.shape[0]
    fields = (
        (n.ka, n.all_ka), (n.va, n.all_va), (n.qa, n.all_qa),
        (n.kb, n.all_kb), (n.vb, n.all_vb), (n.qb, n.all_qb),
    )

    def columns(field, target, head):
        width = target.shape[-1]
        return field.at[:, pl.ds(pl.multiple_of(head * width, width), width)]

    kept = [pltpu.make_async_copy(n.gates.at[at], n.all_gates.at[at], n.m_kept.at[6])]
    for f, (field, target) in enumerate(fields):
        kept.append(pltpu.make_async_copy(columns(field, target, at), target.at[at], n.m_kept.at[f]))
    for copy in kept:
        copy.start()
    went = []
    to, of = partners(at, blocks)
    peers, givers = to[1:], of[1:]
    for step, peer in enumerate(peers):
        went.append(
            send(
                n.gates.at[peer], n.all_gates.at[at], (n.m_sent, n.m_landed), (step, 6),
                {"sp": part * blocks + peer},
            )
        )
    for f, (field, target) in enumerate(fields):
        for step, peer in enumerate(peers):
            went.append(
                send(
                    columns(field, target, peer), target.at[at],
                    (n.m_sent, n.m_landed), (step, f), {"sp": part * blocks + peer},
                )
            )
    near = blocks - 1
    for copy in kept:
        copy.wait()
    for copy in went[:near]:
        copy.wait_recv()
    rows = lax.broadcasted_iota(jnp.int32, (length, length), 0)
    lanes = lax.broadcasted_iota(jnp.int32, (length, length), 1)
    upper = (rows <= lanes).astype(jnp.float32)
    lower = (rows >= lanes).astype(jnp.float32)
    ahead = lax.broadcasted_iota(jnp.int32, (4, 1), 0) < 2
    ahead_lane = lax.broadcasted_iota(jnp.int32, (length, 4), 1) < 2
    tails, wholes = [], []
    for b in range(blocks):
        inputs, decay = n.all_gates[b, 0:4], n.all_gates[b, 4:8]
        run = jnp.where(
            ahead,
            exact_dot(decay, upper, ((1,), (0,))),
            exact_dot(decay, lower, ((1,), (0,))),
        )
        n.column[b] = jnp.where(
            ahead_lane,
            exact_dot(lower, decay, ((1,), (1,))),
            exact_dot(upper, decay, ((1,), (1,))),
        )
        whole = jnp.sum(decay, axis=1, keepdims=True)
        n.inner[b] = inputs - run
        tails.append(inputs + whole - run)
        wholes.append(whole)
    nothing = jnp.zeros((4, 1), jnp.float32)
    before, after = [nothing], [nothing]
    for b in range(blocks - 1):
        before.append(before[-1] + wholes[b])
        after.insert(0, after[0] + wholes[blocks - 1 - b])
    ends = [tails[b] + jnp.where(ahead, after[b], before[b]) for b in range(blocks)]
    peak = functools.reduce(
        jnp.maximum, [jnp.max(logs, axis=1, keepdims=True) for logs in ends]
    )
    first = part == 0
    weights = [jnp.exp(logs - peak) for logs in ends]
    weights = [jnp.where(first, w[0:2], w[2:4]) for w in weights]
    n.note[2:4] = jnp.broadcast_to(jnp.where(first, peak[0:2], peak[2:4]), (2, length))
    for t in range(blocks):
        seen = []
        for b in range(blocks):
            if b < t:
                logs = tails[b] + sum(wholes[b + 1 : t], nothing)
                seen.append(jnp.where(ahead, logs, NOTHING))
            elif b > t:
                logs = tails[b] + sum(wholes[t + 1 : b], nothing)
                seen.append(jnp.where(ahead, NOTHING, logs))
            else:
                seen.append(jnp.full((4, length), NOTHING, jnp.float32))
        top = functools.reduce(
            jnp.maximum, [jnp.max(logs, axis=1, keepdims=True) for logs in seen]
        )
        for b in range(blocks):
            n.outer[t, :, b * length : (b + 1) * length] = jnp.where(
                seen[b] > 0.5 * NOTHING, jnp.exp(seen[b] - top), 0.0
            )
        n.peak[t] = jnp.broadcast_to(top, (4, length))
        n.offset[t] = jnp.broadcast_to(jnp.where(ahead, before[t], after[t]), (4, length))
    other = {"sp": lax.rem(mine + blocks, 2 * blocks)}
    n.note[4:8] = jnp.zeros((4, length), jnp.float32)
    states = []

    def landed(*waves):
        for wave in waves:
            for copy in went[(1 + wave) * near : (2 + wave) * near]:
                copy.wait_recv()

    def state(g):
        keys, values, memory, far = (
            (n.all_ka, n.all_va, n.memory_a, n.far_a), (n.all_kb, n.all_vb, n.memory_b, n.far_b)
        )[g]
        total, normal = None, None
        for b in range(blocks):
            key = keys[b].astype(jnp.float32).T * weights[b][g : g + 1]
            piece = dot(key.astype(jnp.bfloat16), values[b], ((1,), (0,)))
            total = piece if total is None else total + piece
            amount = exact_dot(weights[b], keys[b].astype(jnp.float32), ((1,), (0,)))[g : g + 1]
            normal = amount if normal is None else normal + amount
        memory[...] = total.astype(jnp.bfloat16)
        n.note[g : g + 1] = normal
        states.append(send(memory, far, (n.h_sent, n.h_landed), g, other))

    def local_pass(g, start, stop):
        q, k, v, shut, wide = (
            (n.all_qa, n.all_ka, n.all_va, n.shut_a, n.open_a),
            (n.all_qb, n.all_kb, n.all_vb, n.shut_b, n.open_b),
        )[g]
        scale = q.shape[-1] ** (-0.5)
        order = jnp.where(first, 1, -1)
        keeps = [(rows - lanes) * order >= 0, (lanes - rows) * order >= 0]

        @pl.loop(start, stop)
        def _(turn):
            t = lax.rem(at + 1 + turn, blocks)
            keys = k[...].reshape(blocks * length, k.shape[-1])
            values = v[...].reshape(blocks * length, v.shape[-1])
            near_scores = dot(q[t], k[t], ((1,), (1,))) * scale
            far_scores = dot(q[t], keys, ((1,), (1,))) * scale

            def pick(ref, i):
                ahead_row, behind_row = ref[t, g : g + 1], ref[t, 2 + g : 3 + g]
                if i == 0:
                    return jnp.where(first, ahead_row, behind_row)
                return jnp.where(first, behind_row, ahead_row)

            sums = []
            for i in range(2):
                forth, back = n.column[t, :, g : g + 1], n.column[t, :, 2 + g : 3 + g]
                column = jnp.where(first, forth, back) if i == 0 else jnp.where(first, back, forth)
                sums.append(
                    near_sums(
                        near_scores, far_scores, v[t], values, pick(n.outer, i),
                        pick(n.inner, i), column, pick(n.peak, i)[:, 0:1], keeps[i],
                    )
                )
            shut[t] = settle(*sums[0])
            wide[t] = sums[1][0]
            n.stat[t, :, 2 * g : 2 * g + 1] = sums[1][1]
            n.stat[t, :, 2 * g + 1 : 2 * g + 2] = sums[1][2]

    landed(0, 1)
    state(0)
    landed(2)
    local_pass(0, 0, blocks // 2)
    landed(3, 4)
    state(1)
    states.append(send(n.note, n.far_note, (n.h_sent, n.h_landed), 2, other))
    local_pass(0, blocks // 2, blocks)
    landed(5)
    local_pass(1, 0, blocks)
    for copy in states:
        copy.wait_recv()

    def give(t, g):
        source = (n.out_a, n.out_b)[g]
        target = (n.heads_a, n.heads_b)[g]
        width = source.shape[-1]
        return pltpu.make_async_remote_copy(
            src_ref=source.at[t],
            dst_ref=target.at[:, pl.ds(pl.multiple_of(at * width, width), width)],
            send_sem=n.o_sent.at[t, g],
            recv_sem=n.o_landed.at[at, g],
            device_id={"sp": part * blocks + t},
            device_id_type=MESH,
        )

    def keep(g):
        source = (n.out_a, n.out_b)[g]
        target = (n.heads_a, n.heads_b)[g]
        width = source.shape[-1]
        return pltpu.make_async_copy(
            source.at[at],
            target.at[:, pl.ds(pl.multiple_of(at * width, width), width)],
            n.m_kept.at[7 + g],
        )

    @pl.loop(0, blocks)
    def _(turn):
        t = lax.rem(at + 1 + turn, blocks)
        groups = (
            (n.all_qa, n.far_a, n.gain_a, n.shut_a, n.open_a, n.out_a),
            (n.all_qb, n.far_b, n.gain_b, n.shut_b, n.open_b, n.out_b),
        )
        for g, (q, far, gain, shut, wide, out) in enumerate(groups):
            scale = q.shape[-1] ** (-0.5)
            query = q[t]
            reach = dot(query, far[...], ((1,), (0,))) * scale
            reach_sum = (
                jnp.sum(query.astype(jnp.float32) * n.far_note[g : g + 1], axis=1, keepdims=True)
                * scale
            )
            column = jnp.where(first, n.column[t, :, 2 + g : 3 + g], n.column[t, :, g : g + 1])
            offset = jnp.where(
                first, n.offset[t, 2 + g : 3 + g, 0:1], n.offset[t, g : g + 1, 0:1]
            )
            log = column + offset + n.far_note[2 + g : 3 + g, 0:1]
            denom = n.stat[t, :, 2 * g : 2 * g + 1]
            old = n.stat[t, :, 2 * g + 1 : 2 * g + 2]
            top = jnp.maximum(old, log)
            kept_part, reach_part = jnp.exp(old - top), jnp.exp(log - top)
            both = shut[t] + settle(
                kept_part * wide[t] + reach_part * reach,
                kept_part * denom + reach_part * reach_sum,
                top,
            )
            mean = jnp.mean(both * both, axis=1, keepdims=True)
            out[t] = (
                both * lax.rsqrt(mean + EPSILON) * gain[pl.ds(at, 1), :]
            ).astype(jnp.bfloat16)

            @pl.when(t != at)
            def _():
                give(t, g).start()

    def finish():
        for copy in went:
            copy.wait_send()
        for copy in states:
            copy.wait_send()
        for peer in peers:
            for g in range(2):
                give(peer, g).wait_send()

    for g in range(2):
        keep(g).start()
    for g in range(2):
        keep(g).wait()
    for peer in givers:
        for g in range(2):
            width = (n.out_a, n.out_b)[g].shape[-1]
            pltpu.make_async_remote_copy(
                src_ref=(n.out_a, n.out_b)[g].at[at],
                dst_ref=(n.heads_a, n.heads_b)[g].at[
                    :, pl.ds(pl.multiple_of(peer * width, width), width)
                ],
                send_sem=n.o_sent.at[at, g],
                recv_sem=n.o_landed.at[peer, g],
                device_id={"sp": part * blocks + peer},
                device_id_type=MESH,
            ).wait_recv()
    return finish


def project_part(n, count, across):
    slot = lax.axis_index("tp")
    chips = across // 2
    core, row = lax.rem(slot, 2), lax.div(slot, 2)
    twin = slot + 1 - 2 * core
    width = n.residual.shape[0]
    tokens = n.residual.shape[1]
    slots = n.given.shape[1]
    for copy in n.out_weights:
        copy.wait()

    def block(owner):
        columns = pl.ds(pl.multiple_of(owner * width, width), width)
        return dot(n.heads_a[...], n.wa[:, columns], ((1,), (0,))) + dot(
            n.heads_b[...], n.wb[:, columns], ((1,), (0,))
        )

    to_twin, over = [], []

    def cross(turn):
        to_twin[turn].wait_recv()
        n.mix_chip[turn] = (n.mix_own[turn] + n.mix_in[turn].astype(jnp.float32)).astype(
            jnp.bfloat16
        )
        other = lax.rem(slot + 2 * (turn + 1), across)
        over.append(
            send(n.mix_chip.at[turn], n.mix_far.at[turn], (n.q_sent, n.q_landed), turn, {"tp": other})
        )

    for turn in range(chips):
        y = lax.rem(row + turn + 1, chips)
        n.mix_out[turn] = block(2 * y + 1 - core).astype(jnp.bfloat16)
        to_twin.append(
            send(n.mix_out.at[turn], n.mix_in.at[turn], (n.p_sent, n.p_landed), turn, {"tp": twin})
        )
        if turn > 0:
            cross(turn - 1)
        n.mix_own[turn] = block(2 * y + core)
    experts = lax.broadcasted_iota(jnp.int32, (tokens, 128), 1)
    named = [upright(n.routes[k : k + 1, :]) for k in range(n.routes.shape[0])]
    hits = functools.reduce(jnp.logical_or, [experts == e for e in named])
    earlier = lax.broadcasted_iota(jnp.int32, (tokens, tokens), 0) > lax.broadcasted_iota(
        jnp.int32, (tokens, tokens), 1
    )
    ranks = dot(
        earlier.astype(jnp.float32).astype(jnp.bfloat16),
        hits.astype(jnp.float32).astype(jnp.bfloat16),
        ((1,), (0,)),
    )
    places = lax.broadcasted_iota(jnp.int32, (tokens, count * slots), 1).astype(jnp.float32)
    for k, e in enumerate(named):
        target = jnp.sum(
            jnp.where(experts == e, ranks, 0.0), axis=1, keepdims=True
        ) + e.astype(jnp.float32) * slots
        n.choice[k] = (places == target).astype(jnp.float32).astype(jnp.bfloat16)
    picks = functools.reduce(
        jnp.add, [n.choice[k].astype(jnp.float32) for k in range(len(named))]
    )
    picks = picks.T.astype(jnp.bfloat16)
    base = n.residual[...].astype(jnp.float32).T
    to_twin[chips - 1].wait_recv()
    base = base + (n.mix_own[chips - 1] + n.mix_in[chips - 1].astype(jnp.float32))
    for turn in range(chips - 1):
        over[turn].wait_recv()
        base = base + n.mix_far[turn].astype(jnp.float32)
    n.updated[...] = base
    n.squares[0] = exact_dot(jnp.ones((8, width), jnp.float32), base * base, ((1,), (1,)))
    told = []
    for step in range(1, across):
        told.append(
            send(
                n.squares.at[0], n.squares.at[step], (n.v_sent, n.v_landed), step - 1,
                {"tp": lax.rem(slot + step, across)},
            )
        )
    raw = (n.updated[...] * n.norm_gain[...]).astype(jnp.bfloat16)
    n.given[...] = (
        dot(picks, raw, ((1,), (0,))).astype(jnp.bfloat16).reshape(count, slots, width)
    )

    def spread():
        for copy in told:
            copy.wait_recv()
        squares = n.squares[0]
        for step in range(1, across):
            squares = squares + n.squares[step]
        factor = lax.rsqrt(squares / (width * across) + EPSILON)
        chosen = functools.reduce(
            jnp.add, [n.choice[k].astype(jnp.float32) for k in range(len(named))]
        )
        placed = exact_dot(factor, chosen, ((1,), (0,)))
        n.factor[...] = jnp.zeros(n.factor.shape, jnp.float32)
        for e in range(count):
            n.factor[e, :, 0:slots] = placed[:, e * slots : (e + 1) * slots]

    n.spread = spread

    def finish():
        for copy in to_twin + over + told:
            copy.wait_send()

    return finish


def moe_part(n, count, across):
    mine, slot = lax.axis_index("sp"), lax.axis_index("tp")
    chips = across // 2
    given, rows, hidden, part = n.given, n.rows, n.hidden, n.part
    partner, chip, cross, total, out = n.partner, n.chip, n.cross, n.total, n.returned
    slots, width = given.shape[1], given.shape[2]
    units = n.gate_w.shape[1]
    core = lax.rem(slot, 2)
    row = lax.div(slot, 2)
    twin = slot + 1 - 2 * core
    others = [lax.rem(slot + 2 * step, across) for step in range(1, chips)]
    behind = [lax.rem(slot + across - 2 * step, across) for step in range(1, chips)]
    targets, sources = partners(mine, count)
    order = arrival_order(count)

    scales = {}

    def scale_out():
        n.spread()
        for i in range(1, count):
            step = order[i]
            scales[i] = send(
                n.factor.at[targets[step]], n.factor_in.at[i], (n.f_sent, n.f_landed), i,
                {"sp": targets[step]},
            )
        n.factor_in[0] = n.factor[mine]

    def place(step, owner):
        return rows.at[step, :, pl.ds(pl.multiple_of(owner * width, width), width)]

    first = [pltpu.make_async_copy(given.at[mine], place(0, slot), n.kept.at[0])]
    first[0].start()
    first += [None] * (count - 1)
    for step in order[1:]:
        first[step] = send(
            given.at[targets[step]], place(order.index(step), slot), (n.sent, n.landed), step,
            {"sp": targets[step]},
        )
    along, last = {}, {}

    def relay(i):
        if i == 0:
            first[0].wait()
        else:
            first[order[i]].wait_recv()
        along[i] = [
            send(place(i, slot), place(i, slot), (n.y_sent, n.y_landed), (i, turn), {"tp": other})
            for turn, other in enumerate(others)
        ]
        last[i] = [
            send(place(i, slot), place(i, slot), (n.c_sent, n.c_landed), (i, 0), {"tp": twin})
        ]

    def hand_over(i):
        for turn, owner in enumerate(behind):
            along[i][turn].wait_recv()
            last[i].append(
                send(
                    place(i, owner), place(i, owner), (n.c_sent, n.c_landed),
                    (i, turn + 1), {"tp": twin},
                )
            )

    groups = 4
    span = count // groups
    tile = min(256, units)
    batch = span * slots
    over, crossed, back = {}, {}, {}

    def block(h):
        return pl.ds(h * span, span)

    def arrive(h):
        for i in range(h * span, (h + 1) * span):
            for copy in last[i]:
                copy.wait_recv()

    def lift(h):
        x = rows[h * span : (h + 1) * span].reshape(batch, width * across)
        factors = []
        for i in range(h * span, (h + 1) * span):
            if i > 0:
                scales[i].wait_recv()
            factors.append(upright(n.factor_in[i, 0:1])[0:slots])
        factor = jnp.concatenate(factors, axis=0)
        for turn in range(units // tile):
            columns = slice(turn * tile, (turn + 1) * tile)
            gate = factor * dot(x, n.gate_w[:, columns], ((1,), (0,)))
            upward = factor * dot(x, n.up_w[:, columns], ((1,), (0,)))
            hidden[h * batch : (h + 1) * batch, columns] = (
                jax.nn.silu(gate) * upward
            ).astype(jnp.bfloat16)

    def lower(h):
        x = hidden[h * batch : (h + 1) * batch, :]
        ys = [lax.rem(row + turn + 1, chips) for turn in range(chips)]
        for whose in (1 - core, core):
            for turn, y in enumerate(ys):
                owner = 2 * y + whose
                columns = pl.ds(pl.multiple_of(owner * width, width), width)
                value = dot(x, n.down_w[:, columns], ((1,), (0,)))
                side = 0 if whose is not core else 1
                part[side, turn, block(h)] = value.astype(jnp.bfloat16).reshape(
                    span, slots, width
                )
                if side == 0:
                    over[h, turn] = send(
                        part.at[0, turn, block(h)], partner.at[turn, block(h)],
                        (n.t_sent, n.t_landed), (h, turn), {"tp": twin},
                    )

    def joined(h, turn):
        over[h, turn].wait_recv()
        return part[1, turn, block(h)].astype(jnp.float32) + partner[turn, block(h)].astype(
            jnp.float32
        )

    def join_twin(h):
        for turn in range(chips - 1):
            chip[turn, block(h)] = joined(h, turn).astype(jnp.bfloat16)
            crossed[h, turn] = send(
                chip.at[turn, block(h)], cross.at[turn, block(h)], (n.r_sent, n.r_landed),
                (h, turn), {"tp": others[turn]},
            )

    def give_back(h):
        value = joined(h, chips - 1)
        for turn in range(chips - 1):
            crossed[h, turn].wait_recv()
            value = value + cross[turn, block(h)].astype(jnp.float32)
        total[block(h)] = value.astype(jnp.bfloat16)
        for i in range(h * span, (h + 1) * span):
            step = order[i]
            if step == 0:
                back[step] = pltpu.make_async_copy(total.at[i], out.at[mine], n.kept.at[1])
                back[step].start()
            else:
                back[step] = send(
                    total.at[i], out.at[mine], (n.s_sent, n.s_landed), step,
                    {"sp": sources[step]},
                )

    def weights_in(picked):
        for copy in picked:
            copy.wait()

    tasks = {
        2 * span: [
            functools.partial(weights_in, n.expert_weights[:2]),
            functools.partial(arrive, 0), functools.partial(lift, 0),
        ],
        2 * span + 1: [
            functools.partial(weights_in, n.expert_weights[2:]), functools.partial(lower, 0),
        ],
        3 * span: [
            functools.partial(arrive, 1), functools.partial(lift, 1),
            functools.partial(join_twin, 0), functools.partial(lower, 1),
        ],
    }
    relay(0)
    scale_out()
    for i in range(1, count):
        for task in tasks.get(i, []):
            task()
        relay(i)
        hand_over(i - 1)
    hand_over(count - 1)
    arrive(2)
    lift(2)
    join_twin(1)
    lower(2)
    give_back(0)
    arrive(3)
    join_twin(2)
    lift(3)
    lower(3)
    give_back(1)
    join_twin(3)
    give_back(2)
    give_back(3)
    back[0].wait()
    for i in range(count):
        if i > 0:
            first[i].wait_send()
            back[i].wait()
            scales[i].wait_send()
        for copy in along[i] + last[i]:
            copy.wait_send()
    for copy in list(over.values()) + list(crossed.values()):
        copy.wait_send()


def layer_kernel(count, across, names, mixing, *refs):
    n = Names()
    for name, ref in zip(names, refs):
        setattr(n, name, ref)
    mine, slot = lax.axis_index("sp"), lax.axis_index("tp")
    n.out_weights = [
        pltpu.make_async_copy(source, target, n.weight.at[i])
        for i, (source, target) in enumerate(((n.out_wa, n.wa), (n.out_wb, n.wb)))
    ]
    n.expert_weights = [
        pltpu.make_async_copy(source, target, n.weight.at[2 + i])
        for i, (source, target) in enumerate(
            ((n.gate, n.gate_w), (n.up, n.up_w), (n.down, n.down_w))
        )
    ]
    peers = [{"sp": lax.rem(mine + step, count)} for step in range(1, count)]
    peers += [{"tp": lax.rem(slot + step, across)} for step in range(1, across)]
    barrier = pltpu.get_barrier_semaphore()
    for peer in peers:
        pl.semaphore_signal(barrier, inc=1, device_id=peer, device_id_type=MESH)
    for copy in n.out_weights + n.expert_weights:
        copy.start()
    if mixing:
        gate_part(n)
    pl.semaphore_wait(barrier, len(peers))
    done = []
    if mixing:
        done.append(mixer_part(n))
    done.append(project_part(n, count, across))
    moe_part(n, count, across)
    result = n.updated[...]
    returned = n.returned[...].reshape(-1, n.returned.shape[-1])
    for k in range(n.choice.shape[0]):
        result = result + upright(n.route_weights[k : k + 1, :]) * dot(
            n.choice[k], returned, ((1,), (0,))
        )
    n.out[...] = result.T.astype(jnp.bfloat16)
    for finish in done:
        finish()


def layer(mixer, others, weights, count, across, slots, number):
    bf16, f32 = jnp.bfloat16, jnp.float32
    vmem = pl.BlockSpec(memory_space=pltpu.VMEM)
    whole = pl.BlockSpec(memory_space=pl.ANY)
    dma = pltpu.SemaphoreType.DMA
    chips = across // 2
    width, tokens = others["residual"].shape
    top = others["routes"].shape[0]
    units = weights["gate"].shape[1]
    mixing = "qa" in mixer
    pieces = 4
    scratch = {}

    def buffer(name, shape, dtype=bf16):
        scratch[name] = pltpu.VMEM(shape, dtype)

    def pair(name, shape):
        scratch[name + "_sent"] = dma(shape)
        scratch[name + "_landed"] = dma(shape)

    if mixing:
        blocks = mixer["gain_a"].shape[0]
        wide_a, wide_b = mixer["gain_a"].shape[1], mixer["gain_b"].shape[1]
        dk = mixer["qa"].shape[1] // blocks
        for g, wide in (("a", wide_a), ("b", wide_b)):
            buffer("all_q" + g, (blocks, tokens, dk))
            buffer("all_k" + g, (blocks, tokens, dk))
            buffer("all_v" + g, (blocks, tokens, wide))
            buffer("memory_" + g, (dk, wide))
            buffer("far_" + g, (dk, wide))
            buffer("out_" + g, (blocks, tokens, wide))
            buffer("shut_" + g, (blocks, tokens, wide), f32)
            buffer("open_" + g, (blocks, tokens, wide), f32)
            buffer("heads_" + g, (tokens, blocks * wide))
        buffer("gates", (blocks, 8, tokens), f32)
        buffer("all_gates", (blocks, 8, tokens), f32)
        buffer("note", (8, tokens), f32)
        buffer("far_note", (8, tokens), f32)
        buffer("column", (blocks, tokens, 4), f32)
        buffer("stat", (blocks, tokens, 4), f32)
        buffer("inner", (blocks, 4, tokens), f32)
        buffer("outer", (blocks, 4, blocks * tokens), f32)
        buffer("peak", (blocks, 4, tokens), f32)
        buffer("offset", (blocks, 4, tokens), f32)
        scratch["m_kept"] = dma((9,))
        pair("m", (blocks - 1, 7))
        pair("h", (3,))
        pair("o", (blocks, 2))
    buffer("wa", weights["out_wa"].shape)
    buffer("wb", weights["out_wb"].shape)
    buffer("mix_out", (chips, tokens, width))
    buffer("mix_in", (chips, tokens, width))
    buffer("mix_own", (chips, tokens, width), f32)
    buffer("mix_chip", (chips - 1, tokens, width))
    buffer("mix_far", (chips - 1, tokens, width))
    buffer("updated", (tokens, width), f32)
    buffer("squares", (across, 8, tokens), f32)
    buffer("factor", (count, 8, 128), f32)
    buffer("factor_in", (count, 8, 128), f32)
    pair("f", (count,))
    buffer("choice", (top, tokens, count * slots))
    buffer("given", (count, slots, width))
    buffer("returned", (count, slots, width))
    buffer("rows", (count, slots, width * across))
    buffer("gate_w", weights["gate"].shape)
    buffer("up_w", weights["up"].shape)
    buffer("down_w", weights["down"].shape)
    buffer("hidden", (count * slots, units))
    buffer("part", (2, chips, count, slots, width))
    buffer("partner", (chips, count, slots, width))
    buffer("chip", (chips - 1, count, slots, width))
    buffer("cross", (chips - 1, count, slots, width))
    buffer("total", (count, slots, width))
    scratch["kept"] = dma((2,))
    scratch["weight"] = dma((5,))
    pair("p", (chips,))
    pair("q", (chips - 1,))
    pair("v", (across - 1,))
    scratch["sent"], scratch["landed"] = dma((count,)), dma((count,))
    pair("y", (count, chips - 1))
    pair("c", (count, chips))
    pair("t", (pieces, chips))
    pair("r", (pieces, chips - 1))
    pair("s", (count,))
    inputs = {**mixer, **others, **weights}
    names = list(inputs) + ["out"] + list(scratch)
    return pl.pallas_call(
        functools.partial(layer_kernel, count, across, names, mixing),
        out_shape=jax.ShapeDtypeStruct((width, tokens), bf16),
        in_specs=[whole if name in weights else vmem for name in inputs],
        out_specs=vmem,
        scratch_shapes=list(scratch.values()),
        compiler_params=pltpu.CompilerParams(
            collective_id=number, has_side_effects=True, vmem_limit_bytes=56 * 1024 * 1024
        ),
    )(*inputs.values())


def local(
    query_a,
    key_a,
    value_a,
    query_b,
    key_b,
    value_b,
    in_gate,
    forget_gate,
    head_gain_a,
    head_gain_b,
    out_weight_a,
    out_weight_b,
    residual,
    norm_gain,
    routes,
    route_weights,
    expert_gate,
    expert_up,
    expert_down,
):
    count, across = lax.axis_size("sp"), lax.axis_size("tp")
    heads = head_gain_a.shape[0]
    if 2 * heads == count:
        mixer = dict(
            qa=query_a, ka=key_a, va=value_a, qb=query_b, kb=key_b, vb=value_b,
            in_gate=in_gate, forget_gate=forget_gate, gain_a=head_gain_a, gain_b=head_gain_b,
        )
    else:
        heads_a, heads_b = mix_heads(
            query_a, key_a, value_a, query_b, key_b, value_b,
            in_gate, forget_gate, head_gain_a, head_gain_b,
        )
        mixer = dict(heads_a=heads_a, heads_b=heads_b)
    token_count, top_count = routes.shape
    expert_count = count * expert_gate.shape[0]
    slots = 2 * token_count * top_count // expert_count
    others = dict(
        residual=residual, norm_gain=norm_gain[None, :], routes=routes.T,
        route_weights=route_weights.T,
    )
    weights = dict(
        out_wa=out_weight_a, out_wb=out_weight_b,
        gate=expert_gate[0], up=expert_up[0], down=expert_down[0],
    )
    return layer(mixer, others, weights, count, across, slots, 0)


def solution(mesh):
    placed = (
        P("sp", "tp"),
        P("sp", "tp"),
        P("sp", "tp"),
        P("sp", "tp"),
        P("sp", "tp"),
        P("sp", "tp"),
        P(None, None, "tp", "sp"),
        P(None, None, "tp", "sp"),
        P("tp", None),
        P("tp", None),
        P("tp", None),
        P("tp", None),
        P("tp", "sp"),
        P("tp"),
        P("sp", None),
        P("sp", None),
        P("sp", None, "tp"),
        P("sp", None, "tp"),
        P("sp", "tp", None),
    )
    return jax.shard_map(
        local, mesh=mesh, in_specs=placed, out_specs=P("tp", "sp"), check_vma=False
    )
```
